512 devices in a mesh: gr: 2 (over z_hi), fs: 32 (over z_lo, y), tp: 8 (over x, core).
Axes of the slice: x: 4, y: 4, z: 16 (z_hi: 2, z_lo: 8; z = z_hi * 8 + z_lo), core: 2. Of those that a mesh axis runs over, the one named last changes fastest.
Arguments:
- prompt: bfloat16 [8192, 2048], P(('gr', 'tp'), 'fs'), may hold values from -2.5 to 2.5
- gain_pre: float32 [2048], P(('gr', 'fs')), may hold values from 0.1 to 1.9
- gate_pre: float32 [2048, 5632], P(('gr', 'fs'), 'tp'), may hold values from -6 to 6
- up_pre: float32 [2048, 5632], P(('gr', 'fs'), 'tp'), may hold values from -6 to 6
- down_pre: float32 [2048, 5632], P(('gr', 'fs'), 'tp'), may hold values from -16 to 16
- gain_post: float32 [2048], P(('gr', 'fs')), may hold values from 0.1 to 1.9
- gate_post: float32 [2048, 5632], P(('gr', 'fs'), 'tp'), may hold values from -6 to 6
- up_post: float32 [2048, 5632], P(('gr', 'fs'), 'tp'), may hold values from -6 to 6
- down_post: float32 [2048, 5632], P(('gr', 'fs'), 'tp'), may hold values from -16 to 16
Outputs:
- result: bfloat16 [8192, 2048], P(('gr', 'tp'), 'fs')
- gate_first: bfloat16 [5632, 2048], P('fs')
- up_first: bfloat16 [5632, 2048], P('fs')
- down_first: bfloat16 [5632, 2048], P('fs')
- gate_second: bfloat16 [5632, 2048], P('fs')
- up_second: bfloat16 [5632, 2048], P('fs')
- down_second: bfloat16 [5632, 2048], P('fs')
The draws below stay inside these ranges and needn't reach their ends.
All inputs are finite; a program needn't handle non-finite values.
Results may differ from the reference program's by a relative error of at most 0.028.
Values may be sent and summed in bfloat16 or wider, within the bound.
A program may use at most 64 MiB of HBM per device.

```python
import jax
import jax.numpy as jnp
from jax import lax

D = 2048
FF = 5632
TOKENS = 8192
N_FS = 32


def spiked(entries, key, source, target, parts, factor):
    def block_of(axis_at):
        return (jnp.arange(entries.shape[axis_at]) // (entries.shape[axis_at] // parts)).reshape((-1,) + (1,) * (entries.ndim - 1 - axis_at))

    near = jax.random.permutation(key, parts)[block_of(target)]
    far = (block_of(target) + parts // 2) % parts
    return jnp.where((block_of(source) == near) | (block_of(source) == far), factor * entries, entries)


def block_levels(stream_key, dims, split, smallest, largest):
    factor_of = 1.0
    for axis_at, blocks in split:
        steps = jax.random.uniform(jax.random.fold_in(jax.random.fold_in(stream_key, 6), axis_at), (blocks,), jnp.float32, smallest / len(split), largest / len(split))
        factor_of = factor_of * jnp.repeat(jnp.exp(steps), dims[axis_at] // blocks).reshape((-1,) + (1,) * (len(dims) - 1 - axis_at))
    return factor_of


def gaussian(stream_key, extent, deviation, reach, cuts=(), held_as=jnp.bfloat16):
    array = deviation * jax.random.normal(stream_key, extent, jnp.float32)
    if cuts:
        array = array * block_levels(stream_key, extent, cuts, -0.22, 0.18)
    return jnp.clip(array, -reach, reach).astype(held_as)


def heavy_noise(rng, dims, deviation, reach, cuts, heavy, held_as=jnp.bfloat16):
    entries = deviation * jax.random.normal(rng, dims, jnp.float32)
    if cuts:
        entries = entries * block_levels(rng, dims, cuts, -0.22, 0.18)
    return jnp.clip(spiked(entries, jax.random.fold_in(rng, 3), *heavy), -reach, reach).astype(held_as)


def setup_inputs(seed: int = 0) -> dict:
    keys = jax.random.split(jax.random.key(seed), 10)
    return {
        "prompt": gaussian(keys[0], (TOKENS, D), 0.3, 2.5, ((0, 16), (1, 32))),
        "gain_pre": jnp.clip(1.0 + 0.18 * jax.random.normal(keys[1], (D,), jnp.float32), 0.1, 1.9),
        "gate_pre": gaussian(keys[2], (D, FF), 1.0, 6.0, ((0, 64), (1, 8)), jnp.float32),
        "up_pre": gaussian(keys[3], (D, FF), 1.0, 6.0, ((0, 64), (1, 8)), jnp.float32),
        "down_pre": heavy_noise(keys[4], (D, FF), 1.0, 16.0, ((0, 64), (1, 8)), (1, 0, 64, 4.0), jnp.float32),
        "gain_post": jnp.clip(1.0 + 0.18 * jax.random.normal(keys[5], (D,), jnp.float32), 0.1, 1.9),
        "gate_post": gaussian(keys[6], (D, FF), 1.0, 6.0, ((0, 64), (1, 8)), jnp.float32),
        "up_post": gaussian(keys[7], (D, FF), 1.0, 6.0, ((0, 64), (1, 8)), jnp.float32),
        "down_post": heavy_noise(keys[8], (D, FF), 1.0, 16.0, ((0, 64), (1, 8)), (1, 0, 64, 4.0), jnp.float32),
    }


norm_eps = 1e-06

def fold_gain(gain, matrix):
    return (gain[:, None] * matrix).astype(jnp.bfloat16).T

def half_step(tokens, w_gate, w_up, w_down):
    row_count = tokens.shape[0]
    widened = tokens.astype(jnp.float32)
    row_scale = lax.rsqrt(lax.optimization_barrier(jnp.mean(widened * widened, axis=1)) + norm_eps) * D ** (-0.5)
    gate_sum = jnp.dot(tokens, w_gate.T, preferred_element_type=jnp.float32) * row_scale[:, None]
    up_sum = jnp.dot(tokens, w_up.T, preferred_element_type=jnp.float32) * row_scale[:, None]
    hidden = (jax.nn.silu(gate_sum) * up_sum).astype(jnp.bfloat16)
    group_width = FF // N_FS
    hidden_blocks = jnp.transpose(hidden.reshape(row_count, N_FS, group_width), (1, 0, 2))
    down_blocks = w_down.reshape(N_FS, group_width, D)

    def add_block(running, pair):
        term = jnp.dot(pair[0], pair[1], preferred_element_type=jnp.float32)
        rounded = lax.optimization_barrier(term.astype(jnp.bfloat16))
        return (running + rounded.astype(jnp.float32), None)
    branch, _ = lax.scan(add_block, jnp.zeros((row_count, D), jnp.float32), (hidden_blocks, down_blocks))
    return (widened + 0.5 * FF ** (-0.5) * branch).astype(jnp.bfloat16)

def reference(prompt, gain_pre, gate_pre, up_pre, down_pre, gain_post, gate_post, up_post, down_post):
    gate_first = fold_gain(gain_pre, gate_pre)
    up_first = fold_gain(gain_pre, up_pre)
    down_first = down_pre.astype(jnp.bfloat16).T
    gate_second = fold_gain(gain_post, gate_post)
    up_second = fold_gain(gain_post, up_post)
    down_second = down_post.astype(jnp.bfloat16).T
    middle = half_step(prompt, gate_first, up_first, down_first)
    result = half_step(middle, gate_second, up_second, down_second)
    return (result, gate_first, up_first, down_first, gate_second, up_second, down_second)
```

```python
import jax
import jax.numpy as jnp
from jax import lax
from jax.sharding import PartitionSpec as P

D = 2048
FF = 5632

norm_eps = 1e-06


def half_step(tokens_t, w_gate, w_up, w_down):
    whole = lax.all_gather(tokens_t, "fs", axis=0, tiled=True)
    widened = whole.astype(jnp.float32)
    row_scale = lax.rsqrt(jnp.sum(widened * widened, axis=0, keepdims=True) / D + norm_eps) * D ** (-0.5)
    g = jnp.dot(w_gate, whole, preferred_element_type=jnp.float32) * row_scale
    u = jnp.dot(w_up, whole, preferred_element_type=jnp.float32) * row_scale
    hidden = (jax.nn.silu(g) * u).astype(jnp.bfloat16)
    partial_value = lax.dot_general(w_down, hidden, (((0,), (0,)), ((), ())), preferred_element_type=jnp.float32)
    summed = lax.psum_scatter(partial_value.astype(jnp.bfloat16), "fs", scatter_dimension=0, tiled=True)
    return (tokens_t.astype(jnp.float32) + 0.5 * FF ** (-0.5) * summed.astype(jnp.float32)).astype(jnp.bfloat16)


def relayout(matrices):
    m = jnp.stack(matrices)
    m = m.reshape(6, 8, 4, 704).transpose(1, 0, 2, 3)
    m = lax.all_to_all(m, "tp", 0, 0, tiled=True)
    m = m.reshape(8, 6, 4, 4, 176).transpose(0, 3, 1, 2, 4).reshape(32, 24, 176)
    m = lax.all_to_all(m, "fs", 0, 0, tiled=True)
    m = lax.all_gather(m.reshape(32 * 24, 176), ("gr", "tp"), axis=0, tiled=True)
    m = m.reshape(2, 8, 32, 6, 4, 176).transpose(3, 5, 0, 2, 1, 4).reshape(6, 176, 2048)
    return tuple(m[i] for i in range(6))


def local(prompt, gain_pre, gate_pre, up_pre, down_pre, gain_post, gate_post, up_post, down_post):
    rounded = (
        (gain_pre[:, None] * gate_pre).astype(jnp.bfloat16),
        (gain_pre[:, None] * up_pre).astype(jnp.bfloat16),
        down_pre.astype(jnp.bfloat16),
        (gain_post[:, None] * gate_post).astype(jnp.bfloat16),
        (gain_post[:, None] * up_post).astype(jnp.bfloat16),
        down_post.astype(jnp.bfloat16),
    )
    served = relayout(rounded)
    middle = half_step(prompt.T, served[0], served[1], served[2])
    result = half_step(middle, served[3], served[4], served[5])
    return (result.T, *served)


def solution(mesh):
    rows = P(("gr", "fs"))
    block = P(("gr", "fs"), "tp")
    tokens = P(("gr", "tp"), "fs")
    return jax.shard_map(
        local,
        mesh=mesh,
        in_specs=(tokens, rows, block, block, block, rows, block, block, block),
        out_specs=(tokens,) + (P("fs", None),) * 6,
        check_vma=False,
    )
```

```python
import jax
import jax.numpy as jnp
from jax import lax
from jax.experimental import pallas as pl
from jax.experimental.pallas import tpu as pltpu
from jax.sharding import PartitionSpec as P

D = 2048
FF = 5632
NX, NY, NZ, NG = 4, 4, 8, 2
WIDTH = 176
FEAT = 64
TOK = 512
PART = 144
HALF = NX * PART
NGRP = 4
GCOL = D // NGRP

norm_eps = 1e-06
MESH = pl.DeviceIdType.MESH


def kernel(*refs):
    (x_ref, wp_ref, res_ref, *outs) = refs[:9]
    (xa, xb, pa, pb, ra, rb, r1, tt, r2, wh) = refs[9:19]
    (ag_s, ag_r, rs_s, rs_r, w1_s, w1_r, w2_s, w2_r, w3_s, w3_r, w4_s, w4_r, w5_s, w5_r, out_s) = refs[19:]

    gr, fs, tp = lax.axis_index("gr"), lax.axis_index("fs"), lax.axis_index("tp")
    y, z = lax.rem(fs, NY), fs // NY
    core, x = lax.rem(tp, 2), tp // 2
    zz = gr * NZ + z

    def wrap(v, n):
        return lax.rem(v + n, n)

    def to_y(v):
        return {"fs": z * NY + v}

    def to_z(v):
        return {"fs": v * NY + y}

    def to_zz(v):
        return {"gr": v // NZ, "fs": lax.rem(v, NZ) * NY + y}

    def to_x(v):
        return {"tp": v * 2 + core}

    sibling = {"tp": x * 2 + 1 - core}
    y_up, y_down, y_far = wrap(y + 1, NY), wrap(y - 1, NY), wrap(y + 2, NY)
    x_up, x_down, x_far = wrap(x + 1, NX), wrap(x - 1, NX), wrap(x + 2, NX)

    def remote(src, dst, s, r, to):
        return pltpu.make_async_remote_copy(src, dst, s, r, device_id=to, device_id_type=MESH)

    barrier = pltpu.get_barrier_semaphore()

    def greet_z(i, _):
        pl.semaphore_signal(barrier, inc=1, device_id=to_zz(lax.rem(zz + i, NG * NZ)), device_id_type=MESH)
        return 0

    lax.fori_loop(1, NG * NZ, greet_z, 0)
    for d in range(1, 4):
        pl.semaphore_signal(barrier, inc=1, device_id=to_y(wrap(y + d, NY)), device_id_type=MESH)
        pl.semaphore_signal(barrier, inc=1, device_id=to_x(wrap(x + d, NX)), device_id_type=MESH)
    pl.semaphore_signal(barrier, inc=1, device_id=sibling, device_id_type=MESH)
    pl.semaphore_wait(barrier, NG * NZ - 1 + 3 + 3 + 1)

    ZP, ZM, YP, YM, YF = range(5)

    def gather_copy(k, buf, kind, zs):
        s, r = ag_s.at[k, kind, zs], ag_r.at[k, kind, zs]
        if kind == ZP:
            blk, to = buf.at[zs, y], to_z(jnp.minimum(z + 1, NZ - 1))
        elif kind == ZM:
            blk, to = buf.at[zs, y], to_z(jnp.maximum(z - 1, 0))
        elif kind == YP:
            blk, to = buf.at[zs, y], to_y(y_up)
        else:
            blk, to = buf.at[zs, y], to_y(y_down)
        return remote(blk, blk, s, r, to)

    def relay_up(k, buf, zs):
        blk = buf.at[zs, y_down]
        return remote(blk, blk, ag_s.at[k, YF, zs], ag_r.at[k, YF, zs], to_y(y_up))

    def relay_down(k, buf, zs):
        blk = buf.at[zs, y_up]
        return remote(blk, blk, ag_s.at[k, YF, zs], ag_r.at[k, YF, zs], to_y(y_down))

    def arrived(k, buf, kind, zs, ys):
        blk = buf.at[zs, ys]
        remote(blk, blk, ag_s.at[k, kind, zs], ag_r.at[k, kind, zs], to_y(y_up)).wait_recv()

    def gather_along_z(k, buf, t):
        lower, upper = z - t, z + t

        @pl.when(lower >= 0)
        def _():
            @pl.when(t > 0)
            def _():
                arrived(k, buf, ZP, lower, y)

            @pl.when(z < NZ - 1)
            def _():
                gather_copy(k, buf, ZP, lower).start()

            gather_copy(k, buf, YP, lower).start()
            gather_copy(k, buf, YM, lower).start()

        @pl.when(upper < NZ)
        def _():
            @pl.when(t > 0)
            def _():
                arrived(k, buf, ZM, upper, y)

            @pl.when(z > 0)
            def _():
                gather_copy(k, buf, ZM, upper).start()

            @pl.when(t > 0)
            def _():
                gather_copy(k, buf, YP, upper).start()
                gather_copy(k, buf, YM, upper).start()

    def gather_relay_one(k, buf, zs):
        arrived(k, buf, YP, zs, y_down)

        @pl.when(lax.rem(zs, 2) == 0)
        def _():
            relay_up(k, buf, zs).start()

        arrived(k, buf, YM, zs, y_up)

        @pl.when(lax.rem(zs, 2) == 1)
        def _():
            relay_down(k, buf, zs).start()

    def gather_relay(k, buf, t):
        @pl.when((t >= 0) & (z - t >= 0))
        def _():
            gather_relay_one(k, buf, z - t)

        @pl.when((t > 0) & (z + t < NZ))
        def _():
            gather_relay_one(k, buf, z + t)

    LAG = 2

    def gather_rounds(k, buf, first, last):
        def step(t, _):
            @pl.when(t < NZ)
            def _():
                gather_along_z(k, buf, t)

            gather_relay(k, buf, t - LAG)
            return 0

        lax.fori_loop(first, last, step, 0)

    def gather_end(k, buf):
        def step(zs, _):
            arrived(k, buf, YF, zs, y_far)
            return 0

        lax.fori_loop(0, NZ, step, 0)

    def gather_drain(k, buf):
        def step(zs, _):
            @pl.when((zs <= z) & (z < NZ - 1))
            def _():
                gather_copy(k, buf, ZP, zs).wait_send()

            @pl.when((zs >= z) & (z > 0))
            def _():
                gather_copy(k, buf, ZM, zs).wait_send()

            gather_copy(k, buf, YP, zs).wait_send()
            gather_copy(k, buf, YM, zs).wait_send()
            relay_up(k, buf, zs).wait_send()
            return 0

        lax.fori_loop(0, NZ, step, 0)

    FB, UP, DN = 4, 2, 3

    def send_part(k, part, land, kind, zd, col, to):
        return remote(part.at[zd, col], land.at[kind, zd], rs_s.at[k, kind, zd], rs_r.at[k, kind, zd], to)

    def landed(k, part, land, kind, zd):
        send_part(k, part, land, kind, zd, y, to_y(y_up)).wait_recv()

    def sum_far(k, part, land, zd):
        @pl.when(lax.rem(zd, 2) == 0)
        def _():
            send_part(k, part, land, FB, zd, y_far, to_y(y_up)).start()

        @pl.when(lax.rem(zd, 2) == 1)
        def _():
            send_part(k, part, land, FB, zd, y_far, to_y(y_down)).start()

    def sum_near(k, part, land, zd):
        landed(k, part, land, FB, zd)
        target = jnp.where(lax.rem(zd, 2) == 0, y_up, y_down)
        part[zd, target] = (part[zd, target].astype(jnp.float32) + land[FB, zd].astype(jnp.float32)).astype(jnp.bfloat16)
        send_part(k, part, land, UP, zd, y_up, to_y(y_up)).start()
        send_part(k, part, land, DN, zd, y_down, to_y(y_down)).start()

    def column_sum(k, part, land, zd):
        landed(k, part, land, UP, zd)
        landed(k, part, land, DN, zd)
        return part[zd, y].astype(jnp.float32) + land[UP, zd].astype(jnp.float32) + land[DN, zd].astype(jnp.float32)

    def sum_upward(k, part, land, zd):
        part[zd, y] = column_sum(k, part, land, zd).astype(jnp.bfloat16)

        @pl.when(z > 0)
        def _():
            landed(k, part, land, ZP, zd)
            part[zd, y] = (part[zd, y].astype(jnp.float32) + land[ZP, zd].astype(jnp.float32)).astype(jnp.bfloat16)

        send_part(k, part, land, ZP, zd, y, to_z(jnp.minimum(z + 1, NZ - 1))).start()

    def sum_downward(k, part, land, zd):
        part[zd, y] = column_sum(k, part, land, zd).astype(jnp.bfloat16)

        @pl.when(z < NZ - 1)
        def _():
            landed(k, part, land, ZM, zd)
            part[zd, y] = (part[zd, y].astype(jnp.float32) + land[ZM, zd].astype(jnp.float32)).astype(jnp.bfloat16)

        send_part(k, part, land, ZM, zd, y, to_z(jnp.maximum(z - 1, 0))).start()

    def at_distance(t, f_up, f_down):
        @pl.when((t > 0) & (t < NZ) & (z + t < NZ))
        def _():
            f_up(z + t)

        @pl.when((t >= 0) & (t < NZ) & (z - t >= 0))
        def _():
            f_down(z - t)

    def sum_rounds(k, part, land):
        def step(s, _):
            t = NZ - 1 - s
            at_distance(t, lambda zd: sum_far(k, part, land, zd), lambda zd: sum_far(k, part, land, zd))
            at_distance(t + 1, lambda zd: sum_near(k, part, land, zd), lambda zd: sum_near(k, part, land, zd))
            at_distance(
                jnp.where(t + 2 > 0, t + 2, NZ),
                lambda zd: sum_upward(k, part, land, zd),
                lambda zd: sum_downward(k, part, land, zd),
            )
            return 0

        lax.fori_loop(0, NZ + 1, step, 0)
        total = column_sum(k, part, land, z)
        part[z, y] = total.astype(jnp.bfloat16)

    def sum_result(k, part, land, own):
        sum_rounds(k, part, land)

        @pl.when(z > 0)
        def _():
            landed(k, part, land, ZP, z)

        @pl.when(z < NZ - 1)
        def _():
            landed(k, part, land, ZM, z)

        low = jnp.where(z > 0, land[ZP, z].astype(jnp.float32), 0.0)
        high = jnp.where(z < NZ - 1, land[ZM, z].astype(jnp.float32), 0.0)
        total = part[z, y].astype(jnp.float32) + low + high
        return (own.astype(jnp.float32) + 0.5 * FF ** (-0.5) * total).astype(jnp.bfloat16)

    def sum_drain(k, part, land):
        def step(zd, _):
            for kind in (FB, UP, DN):
                send_part(k, part, land, kind, zd, y, to_y(y_up)).wait_send()

            @pl.when(zd > z)
            def _():
                send_part(k, part, land, ZP, zd, y, to_y(y_up)).wait_send()

            @pl.when(zd < z)
            def _():
                send_part(k, part, land, ZM, zd, y, to_y(y_up)).wait_send()

            return 0

        lax.fori_loop(0, NZ, step, 0)

    def w1_copy(d):
        return remote(
            wp_ref.at[wrap(y + d, NY)], r1.at[pl.ds(y * 32, 32)], w1_s.at[d - 1], w1_r.at[d - 1], to_y(wrap(y + d, NY))
        )

    def w2_copy(h, d):
        xd = wrap(x + d, NX)
        return remote(
            tt.at[pl.ds(pl.multiple_of(h * HALF + xd * PART, 16), PART)],
            r2.at[h, x],
            w2_s.at[h, d - 1],
            w2_r.at[h, d - 1],
            to_x(xd),
        )

    def my_rows(p):
        return pl.ds(pl.multiple_of(p * PART, 16), PART)

    def w3_target(i):
        return lax.rem(i, 2) * NZ + (i // 2) * 2 + core

    def w3_block(h):
        return wh.at[h, my_rows(x), pl.ds(pl.multiple_of(zz * 128, 128), 128)]

    def w3_copy(h, i):
        return remote(r2.at[h, i // 2], w3_block(h), w3_s.at[h, i], w3_r.at[h, zz], to_zz(w3_target(i)))

    def w3_local(h, i):
        return pltpu.make_async_copy(r2.at[h, i // 2], w3_block(h), w3_s.at[h, i])

    def w3_start(h):
        def step(i, _):
            @pl.when(w3_target(i) == zz)
            def _():
                w3_local(h, i).start()

            @pl.when(w3_target(i) != zz)
            def _():
                w3_copy(h, i).start()

            return 0

        lax.fori_loop(0, 2 * NX, step, 0)

    def w3_done(h):
        def step(i, _):
            @pl.when(w3_target(i) == zz)
            def _():
                w3_local(h, i).wait()

            @pl.when(w3_target(i) != zz)
            def _():
                w3_copy(h, i).wait_send()

            return 0

        lax.fori_loop(0, 2 * NX, step, 0)

    def w3_arrive(h, g):
        def step(i, _):
            @pl.when(i != zz)
            def _():
                remote(
                    r2.at[h, 0],
                    wh.at[h, my_rows(x), pl.ds(pl.multiple_of(i * 128, 128), 128)],
                    w3_s.at[h, 0],
                    w3_r.at[h, i],
                    sibling,
                ).wait_recv()

            return 0

        per = NG * NZ // NGRP
        lax.fori_loop(g * per, (g + 1) * per, step, 0)

    def w4_copy(h, kind, p, g, to):
        blk = wh.at[h, my_rows(p), pl.ds(g * GCOL, GCOL)]
        return remote(blk, blk, w4_s.at[h, kind, g], w4_r.at[h, kind, g], to)

    def w5_copy(h, kind, p):
        blk = wh.at[h, my_rows(p)]
        return remote(blk, blk, w5_s.at[h, kind], w5_r.at[h, kind], sibling)

    hub = core == lax.rem(z, 2)

    def w4_send(h):
        w3_done(h)

        @pl.when(hub)
        def _():
            for g in range(NGRP):
                w3_arrive(h, g)
                w4_copy(h, 0, x, g, to_x(x_up)).start()
                w4_copy(h, 1, x, g, to_x(x_down)).start()
            w5_copy(h, 0, x).start()

    def w4_relay(h):
        @pl.when(hub)
        def _():
            for g in range(NGRP):
                w4_copy(h, 0, x_down, g, to_x(x_up)).wait_recv()
                if g % 2 == 0:
                    w4_copy(h, 2, x_down, g, to_x(x_up)).start()
                w4_copy(h, 1, x_up, g, to_x(x_down)).wait_recv()
                if g % 2 == 1:
                    w4_copy(h, 2, x_up, g, to_x(x_down)).start()
            w5_copy(h, 1, x_down).start()
            w5_copy(h, 2, x_up).start()

    def w5_end(h):
        @pl.when(hub)
        def _():
            for g in range(NGRP):
                w4_copy(h, 2, x_far, g, to_x(x_up)).wait_recv()
            w5_copy(h, 3, x_far).start()

        @pl.when(jnp.logical_not(hub))
        def _():
            for kind, p in enumerate((x, x_down, x_up, x_far)):
                w5_copy(h, kind, p).wait_recv()

    def w_drain(h):
        @pl.when(hub)
        def _():
            for kind, p in enumerate((x, x_down, x_up, x_far)):
                w5_copy(h, kind, p).wait_send()
            for kind in range(3):
                for g in range(NGRP):
                    w4_copy(h, kind, x, g, to_x(x_up)).wait_send()

    def out_copy(h, m):
        return pltpu.make_async_copy(wh.at[h, pl.ds(m * WIDTH, WIDTH)], outs[h * 3 + m], out_s.at[h * 3 + m])

    def products(h, buf, part):
        whole = buf[...].reshape(D, TOK)
        wide = whole.astype(jnp.float32)
        squares = jnp.sum(wide * wide, axis=0, keepdims=True)
        row_scale = lax.rsqrt(squares / D + norm_eps) * D ** (-0.5)
        both = jnp.dot(wh[h, 0 : 2 * WIDTH], whole, preferred_element_type=jnp.float32)
        g = both[:WIDTH] * row_scale
        u = both[WIDTH:] * row_scale
        hidden = (g / (1.0 + jnp.exp(-g)) * u).astype(jnp.bfloat16)

        def step(zd, _):
            w = wh[h, 2 * WIDTH : 3 * WIDTH, pl.ds(pl.multiple_of(zd * 256, 256), 256)]
            p = lax.dot_general(w, hidden, (((0,), (0,)), ((), ())), preferred_element_type=jnp.float32)
            part[zd] = p.astype(jnp.bfloat16).reshape(NY, FEAT, TOK)
            return 0

        lax.fori_loop(0, NZ, step, 0)

    for d in range(1, 4):
        w1_copy(d).start()
    xa[z, y] = x_ref[...]
    r1[pl.ds(y * 32, 32), :] = wp_ref[y]
    gather_rounds(0, xa, 0, 1)
    for d in range(1, 4):
        remote(
            wp_ref.at[0], r1.at[pl.ds(wrap(y - d, NY) * 32, 32)], w1_s.at[d - 1], w1_r.at[d - 1], to_y(y_up)
        ).wait_recv()
    for k in range(9):
        tt[k * 128 : (k + 1) * 128, :] = r1[:, k * 128 : (k + 1) * 128].astype(jnp.float32).T.astype(jnp.bfloat16)
    for h in range(2):
        for d in range(1, 4):
            w2_copy(h, d).start()
        r2[h, x] = tt[pl.ds(pl.multiple_of(h * HALF + x * PART, 16), PART), :]

    def w2_wait(h):
        for d in range(1, 4):
            remote(r2.at[h, 0], r2.at[h, wrap(x - d, NX)], w2_s.at[h, d - 1], w2_r.at[h, d - 1], to_x(x_up)).wait_recv()

    gather_rounds(0, xa, 1, 3)
    w2_wait(0)
    w3_start(0)
    gather_rounds(0, xa, 3, NZ + LAG)
    w4_send(0)
    gather_end(0, xa)
    w4_relay(0)
    w5_end(0)
    products(0, xa, pa)
    w2_wait(1)
    w3_start(1)
    for m in range(3):
        out_copy(0, m).start()
    xb[z, y] = sum_result(0, pa, ra, x_ref[...])
    w4_send(1)
    gather_rounds(1, xb, 0, 2)
    w4_relay(1)
    gather_rounds(1, xb, 2, NZ + LAG)
    gather_end(1, xb)
    w5_end(1)
    for m in range(3):
        out_copy(1, m).start()
    products(1, xb, pb)
    res_ref[...] = sum_result(1, pb, rb, xb[z, y])

    for d in range(1, 4):
        w1_copy(d).wait_send()
        for h in range(2):
            w2_copy(h, d).wait_send()
    for h in range(2):
        w_drain(h)
    gather_drain(0, xa)
    gather_drain(1, xb)
    sum_drain(0, pa, ra)
    sum_drain(1, pb, rb)
    for h in range(2):
        for m in range(3):
            out_copy(h, m).wait()


def packed(gate, up, down):
    three = jnp.stack([m.reshape(32, NY, WIDTH) for m in (gate, up, down)], axis=2)
    return jnp.pad(three.reshape(32, NY, 3 * WIDTH), ((0, 0), (0, 0), (0, HALF - 3 * WIDTH)))


def local(prompt, gain_pre, gate_pre, up_pre, down_pre, gain_post, gate_post, up_post, down_post):
    first = packed(
        (gain_pre[:, None] * gate_pre).astype(jnp.bfloat16),
        (gain_pre[:, None] * up_pre).astype(jnp.bfloat16),
        down_pre.astype(jnp.bfloat16),
    )
    second = packed(
        (gain_post[:, None] * gate_post).astype(jnp.bfloat16),
        (gain_post[:, None] * up_post).astype(jnp.bfloat16),
        down_post.astype(jnp.bfloat16),
    )
    wp = jnp.transpose(jnp.concatenate([first, second], axis=2), (1, 0, 2))
    block = jax.ShapeDtypeStruct((WIDTH, D), jnp.bfloat16)
    vm = pl.BlockSpec(memory_space=pltpu.VMEM)
    dma = pltpu.SemaphoreType.DMA
    bf = jnp.bfloat16
    res, *served = pl.pallas_call(
        kernel,
        out_shape=(jax.ShapeDtypeStruct((FEAT, TOK), bf),) + (block,) * 6,
        in_specs=[vm, vm],
        out_specs=(vm,) + (pl.BlockSpec(memory_space=pl.ANY),) * 6,
        scratch_shapes=[
            pltpu.VMEM((NZ, NY, FEAT, TOK), bf),
            pltpu.VMEM((NZ, NY, FEAT, TOK), bf),
            pltpu.VMEM((NZ, NY, FEAT, TOK), bf),
            pltpu.VMEM((NZ, NY, FEAT, TOK), bf),
            pltpu.VMEM((5, NZ, FEAT, TOK), bf),
            pltpu.VMEM((5, NZ, FEAT, TOK), bf),
            pltpu.VMEM((128, 2 * HALF), bf),
            pltpu.VMEM((2 * HALF, 128), bf),
            pltpu.VMEM((2, NX, PART, 128), bf),
            pltpu.VMEM((2, HALF, D), bf),
            dma((2, 5, NZ)),
            dma((2, 5, NZ)),
            dma((2, 5, NZ)),
            dma((2, 5, NZ)),
            dma((3,)),
            dma((3,)),
            dma((2, 3)),
            dma((2, 3)),
            dma((2, 2 * NX)),
            dma((2, NG * NZ)),
            dma((2, 3, NGRP)),
            dma((2, 3, NGRP)),
            dma((2, 4)),
            dma((2, 4)),
            dma((6,)),
        ],
        compiler_params=pltpu.CompilerParams(
            collective_id=0, has_side_effects=True, vmem_limit_bytes=56 * 1024 * 1024
        ),
    )(prompt.T, wp)
    return (res.T, *served)


def solution(mesh):
    rows = P(("gr", "fs"))
    block = P(("gr", "fs"), "tp")
    tokens = P(("gr", "tp"), "fs")
    return jax.shard_map(
        local,
        mesh=mesh,
        in_specs=(tokens, rows, block, block, block, rows, block, block, block),
        out_specs=(tokens,) + (P("fs", None),) * 6,
        check_vma=False,
    )
```

```python
import jax
import jax.numpy as jnp
from jax import lax
from jax.experimental import pallas as pl
from jax.experimental.pallas import tpu as pltpu
from jax.sharding import PartitionSpec as P

D = 2048
FF = 5632
NX, NY, NZ, NG = 4, 4, 8, 2
WIDTH = 176
FEAT = 64
TOK = 512
PART = 48
ROWS = NX * PART
NGRP = 2
GCOL = D // NGRP
EXPRESS = 4

norm_eps = 1e-06
MESH = pl.DeviceIdType.MESH


def kernel(
    x_ref, gain_a, gain_b, *refs
):
    mats, res_ref, outs = refs[:6], refs[6], refs[7:13]
    (xa, xb, pa, pb, ra, rb, wp, r1, tt, r2, wh, gains, loaded) = refs[13:26]
    (ag_s, ag_r, rs_s, rs_r, w1_s, w1_r, w2_s, w2_r, w3_s, w3_r, w4_s, w4_r, w5_s, w5_r, in_s, out_s) = refs[26:]

    gr, fs, tp = lax.axis_index("gr"), lax.axis_index("fs"), lax.axis_index("tp")
    y, z = lax.rem(fs, NY), fs // NY
    core, x = lax.rem(tp, 2), tp // 2
    zz = gr * NZ + z

    loads = [pltpu.make_async_copy(m, loaded.at[i], in_s.at[i]) for i, m in enumerate(mats)]
    loads.append(pltpu.make_async_copy(gain_a, gains.at[0], in_s.at[6]))
    loads.append(pltpu.make_async_copy(gain_b, gains.at[1], in_s.at[7]))
    loads.append(pltpu.make_async_copy(x_ref, xa.at[z, y], in_s.at[8]))
    for c in loads:
        c.start()

    def wrap(v, n):
        return lax.rem(v + n, n)

    def to_y(v):
        return {"fs": z * NY + v}

    def to_z(v):
        return {"fs": v * NY + y}

    def to_zz(v):
        return {"gr": v // NZ, "fs": lax.rem(v, NZ) * NY + y}

    def to_x(v):
        return {"tp": v * 2 + core}

    sibling = {"tp": x * 2 + 1 - core}
    y_up, y_down, y_far = wrap(y + 1, NY), wrap(y - 1, NY), wrap(y + 2, NY)
    x_up, x_down, x_far = wrap(x + 1, NX), wrap(x - 1, NX), wrap(x + 2, NX)

    def remote(src, dst, s, r, to):
        return pltpu.make_async_remote_copy(src, dst, s, r, device_id=to, device_id_type=MESH)

    barrier = pltpu.get_barrier_semaphore()

    def greet_z(i, _):
        pl.semaphore_signal(barrier, inc=1, device_id=to_zz(lax.rem(zz + i, NG * NZ)), device_id_type=MESH)
        return 0

    lax.fori_loop(1, NG * NZ, greet_z, 0)
    for d in range(1, 4):
        pl.semaphore_signal(barrier, inc=1, device_id=to_y(wrap(y + d, NY)), device_id_type=MESH)
        pl.semaphore_signal(barrier, inc=1, device_id=to_x(wrap(x + d, NX)), device_id_type=MESH)
    pl.semaphore_signal(barrier, inc=1, device_id=sibling, device_id_type=MESH)

    def pack(h):
        eye = lax.broadcasted_iota(jnp.int32, (32, 32), 0) == lax.broadcasted_iota(jnp.int32, (32, 32), 1)
        gain = jnp.sum(jnp.where(eye, jnp.broadcast_to(gains[h], (32, 32)), 0.0), axis=1, keepdims=True)
        for m in range(3):
            v = loaded[h * 3 + m]
            v = v * gain if m < 2 else v
            for at in range(NY):
                piece = jnp.pad(v[:, at * WIDTH : (at + 1) * WIDTH], ((0, 0), (0, ROWS - WIDTH)))
                wp[h, at, :, m * ROWS : (m + 1) * ROWS] = piece.astype(jnp.bfloat16)

    for c in loads:
        c.wait()
    pack(0)
    pack(1)
    for h in range(2):
        r1[h, pl.ds(y * 32, 32), :] = wp[h, y]
    pl.semaphore_wait(barrier, NG * NZ - 1 + 3 + 3 + 1)

    STEPS = 6

    def each(s, f_low, f_high):
        d1 = s + jnp.where(s >= 4, 2, 0)
        fits = (s >= 0) & (s < STEPS)

        @pl.when(fits & (z - d1 >= 0))
        def _():
            f_low(z - d1, d1)

        @pl.when(fits & (d1 > 0) & (z + d1 < NZ))
        def _():
            f_high(z + d1, d1)

        d2 = s + 2
        second = (s == 2) | (s == 3)

        @pl.when(second & (z - d2 >= 0))
        def _():
            f_low(z - d2, d2)

        @pl.when(second & (z + d2 < NZ))
        def _():
            f_high(z + d2, d2)

    z_up, z_down = jnp.minimum(z + 1, NZ - 1), jnp.maximum(z - 1, 0)
    z_far_up, z_far_down = jnp.minimum(z + EXPRESS, NZ - 1), jnp.maximum(z - EXPRESS, 0)

    ZP, ZM, UP, DN, FB, XP, XM = range(7)

    def block_copy(k, buf, kind, zs, ys, to, s_kind=None):
        blk = buf.at[zs, ys]
        s_kind = kind if s_kind is None else s_kind
        return remote(blk, blk, ag_s.at[k, s_kind, zs], ag_r.at[k, kind, zs], to)

    def arrived(k, buf, kind, zs, ys):
        block_copy(k, buf, kind, zs, ys, to_y(y_up)).wait_recv()

    def along_y(k, buf, zs):
        block_copy(k, buf, UP, zs, y, to_y(y_up)).start()
        block_copy(k, buf, DN, zs, y, to_y(y_down)).start()

    def gather_low(k, buf, zs, d):
        @pl.when(d > 0)
        def _():
            arrived(k, buf, ZP, zs, y)

        @pl.when((z < NZ - 1) & (d != EXPRESS - 1))
        def _():
            block_copy(k, buf, ZP, zs, y, to_z(z_up)).start()

        @pl.when(d == 0)
        def _():
            @pl.when(z > 0)
            def _():
                block_copy(k, buf, ZM, zs, y, to_z(z_down)).start()

            @pl.when(z + EXPRESS < NZ)
            def _():
                block_copy(k, buf, ZP, zs, y, to_z(z_far_up), XP).start()

            @pl.when(z - EXPRESS >= 0)
            def _():
                block_copy(k, buf, ZM, zs, y, to_z(z_far_down), XM).start()

        along_y(k, buf, zs)

    def gather_high(k, buf, zs, d):
        arrived(k, buf, ZM, zs, y)

        @pl.when((z > 0) & (d != EXPRESS - 1))
        def _():
            block_copy(k, buf, ZM, zs, y, to_z(z_down)).start()

        along_y(k, buf, zs)

    def gather_relay(k, buf, zs):
        arrived(k, buf, UP, zs, y_down)

        @pl.when(lax.rem(zs, 2) == 0)
        def _():
            block_copy(k, buf, FB, zs, y_down, to_y(y_up)).start()

        arrived(k, buf, DN, zs, y_up)

        @pl.when(lax.rem(zs, 2) == 1)
        def _():
            block_copy(k, buf, FB, zs, y_up, to_y(y_down)).start()

    LAG = 2

    def gather_rounds(k, buf, first, last):
        def step(s, _):
            each(s, lambda zs, d: gather_low(k, buf, zs, d), lambda zs, d: gather_high(k, buf, zs, d))
            each(s - LAG, lambda zs, d: gather_relay(k, buf, zs), lambda zs, d: gather_relay(k, buf, zs))
            return 0

        lax.fori_loop(first, last, step, 0)

    def gather_end(k, buf):
        def step(zs, _):
            arrived(k, buf, FB, zs, y_far)
            return 0

        lax.fori_loop(0, NZ, step, 0)

    def gather_drain(k, buf):
        def sent(kind, zs):
            block_copy(k, buf, kind, zs, y, to_y(y_up)).wait_send()

        def step(zs, _):
            @pl.when((zs <= z) & (z < NZ - 1) & (z - zs != EXPRESS - 1))
            def _():
                sent(ZP, zs)

            @pl.when((zs >= z) & (z > 0) & (zs - z != EXPRESS - 1))
            def _():
                sent(ZM, zs)

            sent(UP, zs)
            sent(DN, zs)
            sent(FB, zs)
            return 0

        lax.fori_loop(0, NZ, step, 0)

        @pl.when(z + EXPRESS < NZ)
        def _():
            sent(XP, z)

        @pl.when(z - EXPRESS >= 0)
        def _():
            sent(XM, z)

    def send_part(k, part, land, kind, zd, col, to):
        return remote(part.at[zd, col], land.at[kind, zd], rs_s.at[k, kind, zd], rs_r.at[k, kind, zd], to)

    def landed(k, part, land, kind, zd):
        send_part(k, part, land, kind, zd, y, to_y(y_up)).wait_recv()

    def sum_far(k, part, land, zd):
        @pl.when(lax.rem(zd, 2) == 0)
        def _():
            send_part(k, part, land, FB, zd, y_far, to_y(y_up)).start()

        @pl.when(lax.rem(zd, 2) == 1)
        def _():
            send_part(k, part, land, FB, zd, y_far, to_y(y_down)).start()

    def sum_near(k, part, land, zd):
        landed(k, part, land, FB, zd)
        target = jnp.where(lax.rem(zd, 2) == 0, y_up, y_down)
        part[zd, target] = (part[zd, target].astype(jnp.float32) + land[FB, zd].astype(jnp.float32)).astype(jnp.bfloat16)
        send_part(k, part, land, UP, zd, y_up, to_y(y_up)).start()
        send_part(k, part, land, DN, zd, y_down, to_y(y_down)).start()

    def column_sum(k, part, land, zd):
        landed(k, part, land, UP, zd)
        landed(k, part, land, DN, zd)
        return part[zd, y].astype(jnp.float32) + land[UP, zd].astype(jnp.float32) + land[DN, zd].astype(jnp.float32)

    def sum_along_z(k, part, land, zd, d, chain, express, more, to_next, to_far):
        own = column_sum(k, part, land, zd)

        @pl.when(jnp.logical_not(more & (d != EXPRESS - 1)))
        def _():
            part[zd, y] = own.astype(jnp.bfloat16)

        @pl.when(more & (d != EXPRESS - 1))
        def _():
            landed(k, part, land, chain, zd)
            part[zd, y] = (own + land[chain, zd].astype(jnp.float32)).astype(jnp.bfloat16)

        @pl.when(d != EXPRESS)
        def _():
            send_part(k, part, land, chain, zd, y, to_next).start()

        @pl.when(d == EXPRESS)
        def _():
            send_part(k, part, land, express, zd, y, to_far).start()

    def sum_upward(k, part, land, zd, d):
        sum_along_z(k, part, land, zd, d, ZP, XP, z > 0, to_z(z_up), to_z(z_far_up))

    def sum_downward(k, part, land, zd, d):
        @pl.when(d > 0)
        def _():
            sum_along_z(k, part, land, zd, d, ZM, XM, z < NZ - 1, to_z(z_down), to_z(z_far_down))

    def sum_result(k, part, land, own):
        def step(i, _):
            s = STEPS - 1 - i
            each(s, lambda zd, d: sum_far(k, part, land, zd), lambda zd, d: sum_far(k, part, land, zd))
            each(s + 1, lambda zd, d: sum_near(k, part, land, zd), lambda zd, d: sum_near(k, part, land, zd))
            each(
                s + 2,
                lambda zd, d: sum_downward(k, part, land, zd, d),
                lambda zd, d: sum_upward(k, part, land, zd, d),
            )
            return 0

        lax.fori_loop(0, STEPS + 1, step, 0)
        total = column_sum(k, part, land, z)
        for kind, there in ((ZP, z > 0), (ZM, z < NZ - 1), (XP, z - EXPRESS >= 0), (XM, z + EXPRESS < NZ)):

            @pl.when(there)
            def _(kind=kind):
                landed(k, part, land, kind, z)

            @pl.when(jnp.logical_not(there))
            def _(kind=kind):
                land[kind, z] = jnp.zeros((FEAT, TOK), jnp.bfloat16)

            total = total + land[kind, z].astype(jnp.float32)
        return (own.astype(jnp.float32) + 0.5 * FF ** (-0.5) * total).astype(jnp.bfloat16)

    def sum_drain(k, part, land):
        def sent(kind, zd):
            send_part(k, part, land, kind, zd, y, to_y(y_up)).wait_send()

        def step(zd, _):
            for kind in (FB, UP, DN):
                sent(kind, zd)

            @pl.when((zd > z) & (zd - z != EXPRESS))
            def _():
                sent(ZP, zd)

            @pl.when((zd < z) & (z - zd != EXPRESS))
            def _():
                sent(ZM, zd)

            return 0

        lax.fori_loop(0, NZ, step, 0)

        @pl.when(z + EXPRESS < NZ)
        def _():
            sent(XP, z + EXPRESS)

        @pl.when(z - EXPRESS >= 0)
        def _():
            sent(XM, z - EXPRESS)

    def w1_copy(h, d):
        yd = wrap(y + d, NY)
        return remote(wp.at[h, yd], r1.at[h, pl.ds(y * 32, 32)], w1_s.at[h, d - 1], w1_r.at[h, d - 1], to_y(yd))

    def w1_start(h):
        for d in range(1, NY):
            w1_copy(h, d).start()

    def w1_wait(h):
        for d in range(1, NY):
            rows = pl.ds(wrap(y - d, NY) * 32, 32)
            remote(wp.at[h, 0], r1.at[h, rows], w1_s.at[h, d - 1], w1_r.at[h, d - 1], to_y(y_up)).wait_recv()

    def turn(h):
        turned = r1[h].astype(jnp.float32).T.astype(jnp.bfloat16)
        tt[h] = turned.reshape(3, NX, PART, 128)

    def w2_copy(h, d):
        xd = wrap(x + d, NX)
        return remote(tt.at[h, :, xd], r2.at[h, x], w2_s.at[h, d - 1], w2_r.at[h, d - 1], to_x(xd))

    def w2_start(h):
        for d in range(1, NX):
            w2_copy(h, d).start()
        r2[h, x] = tt[h, :, x]

    def w2_wait(h):
        for d in range(1, NX):
            xs = wrap(x - d, NX)
            remote(r2.at[h, 0], r2.at[h, xs], w2_s.at[h, d - 1], w2_r.at[h, d - 1], to_x(x_up)).wait_recv()

    def part_rows(p):
        return pl.ds(pl.multiple_of(p * PART, 16), PART)

    def w3_block(m, at):
        return wh.at[m, part_rows(x), pl.ds(pl.multiple_of(at * 128, 128), 128)]

    def w3_target(i):
        return lax.rem(i, 2) * NZ + (i // 2) * 2 + core

    def w3_copy(m, i):
        src = r2.at[m // 3, i // 2, m % 3]
        return remote(src, w3_block(m, zz), w3_s.at[m, i], w3_r.at[m, zz], to_zz(w3_target(i)))

    def w3_local(m, i):
        return pltpu.make_async_copy(r2.at[m // 3, i // 2, m % 3], w3_block(m, zz), w3_s.at[m, i])

    def w3_each(m, f_local, f_remote):
        def step(i, _):
            @pl.when(w3_target(i) == zz)
            def _():
                f_local(w3_local(m, i))

            @pl.when(w3_target(i) != zz)
            def _():
                f_remote(w3_copy(m, i))

            return 0

        lax.fori_loop(0, 2 * NX, step, 0)

    def w3_start(m):
        w3_each(m, lambda c: c.start(), lambda c: c.start())

    def w3_arrive(m):
        def step(i, _):
            @pl.when(i != zz)
            def _():
                remote(r2.at[0, 0, 0], w3_block(m, i), w3_s.at[m, 0], w3_r.at[m, i], sibling).wait_recv()

            return 0

        lax.fori_loop(0, NG * NZ, step, 0)

    def w4_copy(m, kind, p, g, to):
        blk = wh.at[m, part_rows(p), pl.ds(g * GCOL, GCOL)]
        return remote(blk, blk, w4_s.at[m, kind, g], w4_r.at[m, kind, g], to)

    def w5_copy(m, kind, p):
        blk = wh.at[m, part_rows(p)]
        return remote(blk, blk, w5_s.at[m, kind], w5_r.at[m, kind], sibling)

    hub = core == lax.rem(z, 2)
    parts = ((0, x), (1, x_down), (2, x_up), (3, x_far))

    def w4_send(m):
        w3_each(m, lambda c: c.wait(), lambda c: c.wait_send())

        @pl.when(hub)
        def _():
            w3_arrive(m)
            for g in range(NGRP):
                w4_copy(m, 0, x, g, to_x(x_up)).start()
                w4_copy(m, 1, x, g, to_x(x_down)).start()
            w5_copy(m, 0, x).start()

    def w4_relay(m):
        @pl.when(hub)
        def _():
            for g in range(NGRP):
                w4_copy(m, 0, x_down, g, to_x(x_up)).wait_recv()
                if g % 2 == 0:
                    w4_copy(m, 2, x_down, g, to_x(x_up)).start()
                w4_copy(m, 1, x_up, g, to_x(x_down)).wait_recv()
                if g % 2 == 1:
                    w4_copy(m, 2, x_up, g, to_x(x_down)).start()
            w5_copy(m, 1, x_down).start()
            w5_copy(m, 2, x_up).start()

    def w5_send(m):
        @pl.when(hub)
        def _():
            for g in range(NGRP):
                w4_copy(m, 2, x_far, g, to_x(x_up)).wait_recv()
            w5_copy(m, 3, x_far).start()

    def w5_wait(m):
        @pl.when(jnp.logical_not(hub))
        def _():
            for kind, p in parts:
                w5_copy(m, kind, p).wait_recv()

    def w_drain():
        @pl.when(hub)
        def _():
            for m in range(6):
                for kind, p in parts:
                    w5_copy(m, kind, p).wait_send()
                for kind in range(3):
                    for g in range(NGRP):
                        w4_copy(m, kind, x, g, to_x(x_up)).wait_send()

    def out_copy(m):
        return pltpu.make_async_copy(wh.at[m, pl.ds(0, WIDTH)], outs[m], out_s.at[m])

    def products(h, buf, part):
        whole = buf[...].reshape(D, TOK)
        wide = whole.astype(jnp.float32)
        squares = jnp.sum(wide * wide, axis=0, keepdims=True)
        row_scale = lax.rsqrt(squares / D + norm_eps) * D ** (-0.5)
        g = jnp.dot(wh[3 * h, 0:WIDTH], whole, preferred_element_type=jnp.float32) * row_scale
        u = jnp.dot(wh[3 * h + 1, 0:WIDTH], whole, preferred_element_type=jnp.float32) * row_scale
        hidden = (g / (1.0 + jnp.exp(-g)) * u).astype(jnp.bfloat16)

        def step(zd, _):
            w = wh[3 * h + 2, 0:WIDTH, pl.ds(pl.multiple_of(zd * 256, 256), 256)]
            p = lax.dot_general(w, hidden, (((0,), (0,)), ((), ())), preferred_element_type=jnp.float32)
            part[zd] = p.astype(jnp.bfloat16).reshape(NY, FEAT, TOK)
            return 0

        lax.fori_loop(0, NZ, step, 0)

    w1_start(0)
    gather_rounds(0, xa, 0, 1)
    w1_start(1)
    w1_wait(0)
    turn(0)
    w2_start(0)
    gather_rounds(0, xa, 1, 2)
    w2_wait(0)
    for m in range(3):
        w3_start(m)
    gather_rounds(0, xa, 2, 3)
    w1_wait(1)
    turn(1)
    w2_start(1)
    gather_rounds(0, xa, 3, STEPS)
    w4_send(0)
    gather_rounds(0, xa, STEPS, STEPS + LAG)
    w4_send(1)
    w4_relay(0)
    w4_send(2)
    w4_relay(1)
    w5_send(0)
    gather_end(0, xa)
    w4_relay(2)
    w5_send(1)
    w5_send(2)
    w2_wait(1)
    for m in range(3, 6):
        w3_start(m)
    for m in range(3):
        w5_wait(m)
    for m in range(3):
        out_copy(m).start()
    products(0, xa, pa)
    xb[z, y] = sum_result(0, pa, ra, xa[z, y])
    gather_rounds(1, xb, 0, 1)
    for m in range(3, 6):
        w4_send(m)
    gather_rounds(1, xb, 1, 3)
    for m in range(3, 6):
        w4_relay(m)
    gather_rounds(1, xb, 3, STEPS)
    for m in range(3, 6):
        w5_send(m)
    gather_rounds(1, xb, STEPS, STEPS + LAG)
    gather_end(1, xb)
    for m in range(3, 6):
        w5_wait(m)
    for m in range(3, 6):
        out_copy(m).start()
    products(1, xb, pb)
    res_ref[...] = sum_result(1, pb, rb, xb[z, y])

    for h in range(2):
        for d in range(1, 4):
            w1_copy(h, d).wait_send()
            w2_copy(h, d).wait_send()
    w_drain()
    for m in range(6):
        out_copy(m).wait()
    gather_drain(0, xa)
    gather_drain(1, xb)
    sum_drain(0, pa, ra)
    sum_drain(1, pb, rb)


def write_out(*refs):
    ins, outs, held, sems = refs[:7], refs[7:14], refs[14:21], refs[21]
    loads = [pltpu.make_async_copy(ins[i], held[i], sems.at[0, i]) for i in range(7)]
    stores = [pltpu.make_async_copy(held[i], outs[i], sems.at[1, i]) for i in range(7)]
    for c in loads:
        c.start()
    for i in range(7):
        loads[i].wait()
        stores[i].start()
    for c in stores:
        c.wait()


def local(prompt, gain_pre, gate_pre, up_pre, down_pre, gain_post, gate_post, up_post, down_post):
    vm = pl.BlockSpec(memory_space=pltpu.VMEM)
    dma = pltpu.SemaphoreType.DMA
    bf = jnp.bfloat16
    hbm = pl.BlockSpec(memory_space=pltpu.HBM)
    shapes = (jax.ShapeDtypeStruct((FEAT, TOK), bf),) + (jax.ShapeDtypeStruct((WIDTH, D), bf),) * 6
    made = pl.pallas_call(
        kernel,
        out_shape=shapes,
        in_specs=[hbm] * 9,
        out_specs=(vm,) + (hbm,) * 6,
        scratch_shapes=[
            pltpu.VMEM((NZ, NY, FEAT, TOK), bf),
            pltpu.VMEM((NZ, NY, FEAT, TOK), bf),
            pltpu.VMEM((NZ, NY, FEAT, TOK), bf),
            pltpu.VMEM((NZ, NY, FEAT, TOK), bf),
            pltpu.VMEM((7, NZ, FEAT, TOK), bf),
            pltpu.VMEM((7, NZ, FEAT, TOK), bf),
            pltpu.VMEM((2, NY, 32, 3 * ROWS), bf),
            pltpu.VMEM((2, 128, 3 * ROWS), bf),
            pltpu.VMEM((2, 3, NX, PART, 128), bf),
            pltpu.VMEM((2, NX, 3, PART, 128), bf),
            pltpu.VMEM((6, ROWS, D), bf),
            pltpu.VMEM((2, 1, 32), jnp.float32),
            pltpu.VMEM((6, 32, NY * WIDTH), jnp.float32),
            dma((2, 7, NZ)),
            dma((2, 7, NZ)),
            dma((2, 7, NZ)),
            dma((2, 7, NZ)),
            dma((2, 3)),
            dma((2, 3)),
            dma((2, 3)),
            dma((2, 3)),
            dma((6, 2 * NX)),
            dma((6, NG * NZ)),
            dma((6, 3, NGRP)),
            dma((6, 3, NGRP)),
            dma((6, 4)),
            dma((6, 4)),
            dma((9,)),
            dma((6,)),
        ],
        compiler_params=pltpu.CompilerParams(
            collective_id=0, has_side_effects=True, vmem_limit_bytes=58 * 1024 * 1024
        ),
    )(
        prompt.T,
        gain_pre.reshape(1, 32),
        gain_post.reshape(1, 32),
        gate_pre,
        up_pre,
        down_pre,
        gate_post,
        up_post,
        down_post,
    )
    res, *served = pl.pallas_call(
        write_out,
        out_shape=shapes,
        in_specs=[hbm] * 7,
        out_specs=(hbm,) * 7,
        scratch_shapes=[pltpu.VMEM(a.shape, bf) for a in shapes] + [dma((2, 7))],
    )(*made)
    return (res.T, *served)


def solution(mesh):
    rows = P(("gr", "fs"))
    block = P(("gr", "fs"), "tp")
    tokens = P(("gr", "tp"), "fs")
    return jax.shard_map(
        local,
        mesh=mesh,
        in_specs=(tokens, rows, block, block, block, rows, block, block, block),
        out_specs=(tokens,) + (P("fs", None),) * 6,
        check_vma=False,
    )
```

```python
import jax
import jax.numpy as jnp
from jax import lax
from jax.experimental import pallas as pl
from jax.experimental.pallas import tpu as pltpu
from jax.sharding import PartitionSpec as P

D = 2048
FF = 5632
NX, NY, NZ, NG = 4, 4, 8, 2
WIDTH = 176
FEAT = 64
TOK = 512
PART = 48
ROWS = NX * PART
NGRP = 2
GCOL = D // NGRP
EXPRESS = 4

norm_eps = 1e-06
MESH = pl.DeviceIdType.MESH


def kernel(
    x_ref, gain_a, gain_b, *refs
):
    mats, res_ref, outs = refs[:6], refs[6], refs[7:13]
    (xa, xb, pa, pb, ra, rb, wp, r1, tt, r2, wh, gains, loaded, hid) = refs[13:27]
    (ag_s, ag_r, rs_s, rs_r, w1_s, w1_r, w2_s, w2_r, w3_s, w3_r, w4_s, w4_r, w5_s, w5_r, in_s, out_s) = refs[27:]
    HALVES = [(c, pl.ds(32 * c, 32)) for c in range(2)]

    gr, fs, tp = lax.axis_index("gr"), lax.axis_index("fs"), lax.axis_index("tp")
    y, z = lax.rem(fs, NY), fs // NY
    core, x = lax.rem(tp, 2), tp // 2
    zz = gr * NZ + z

    loads = [pltpu.make_async_copy(m, loaded.at[i], in_s.at[i]) for i, m in enumerate(mats)]
    loads.append(pltpu.make_async_copy(gain_a, gains.at[0], in_s.at[6]))
    loads.append(pltpu.make_async_copy(gain_b, gains.at[1], in_s.at[7]))
    loads.append(pltpu.make_async_copy(x_ref, xa.at[z, y], in_s.at[8]))
    for c in loads:
        c.start()

    def wrap(v, n):
        return lax.rem(v + n, n)

    def to_y(v):
        return {"fs": z * NY + v}

    def to_z(v):
        return {"fs": v * NY + y}

    def to_zz(v):
        return {"gr": v // NZ, "fs": lax.rem(v, NZ) * NY + y}

    def to_x(v):
        return {"tp": v * 2 + core}

    sibling = {"tp": x * 2 + 1 - core}
    y_up, y_down, y_far = wrap(y + 1, NY), wrap(y - 1, NY), wrap(y + 2, NY)
    x_up, x_down, x_far = wrap(x + 1, NX), wrap(x - 1, NX), wrap(x + 2, NX)

    def remote(src, dst, s, r, to):
        return pltpu.make_async_remote_copy(src, dst, s, r, device_id=to, device_id_type=MESH)

    barrier = pltpu.get_barrier_semaphore()

    def greet_z(i, _):
        pl.semaphore_signal(barrier, inc=1, device_id=to_zz(lax.rem(zz + i, NG * NZ)), device_id_type=MESH)
        return 0

    lax.fori_loop(1, NG * NZ, greet_z, 0)
    for d in range(1, 4):
        pl.semaphore_signal(barrier, inc=1, device_id=to_y(wrap(y + d, NY)), device_id_type=MESH)
        pl.semaphore_signal(barrier, inc=1, device_id=to_x(wrap(x + d, NX)), device_id_type=MESH)
    pl.semaphore_signal(barrier, inc=1, device_id=sibling, device_id_type=MESH)

    def pack(h):
        eye = lax.broadcasted_iota(jnp.int32, (32, 32), 0) == lax.broadcasted_iota(jnp.int32, (32, 32), 1)
        gain = jnp.sum(jnp.where(eye, jnp.broadcast_to(gains[h], (32, 32)), 0.0), axis=1, keepdims=True)
        for m in range(3):
            v = loaded[h * 3 + m]
            v = v * gain if m < 2 else v
            for at in range(NY):
                piece = jnp.pad(v[:, at * WIDTH : (at + 1) * WIDTH], ((0, 0), (0, ROWS - WIDTH)))
                wp[h, at, :, m * ROWS : (m + 1) * ROWS] = piece.astype(jnp.bfloat16)

    for c in loads:
        c.wait()
    pack(0)
    pack(1)
    for h in range(2):
        r1[h, pl.ds(y * 32, 32), :] = wp[h, y]
    pl.semaphore_wait(barrier, NG * NZ - 1 + 3 + 3 + 1)

    STEPS = 6

    def each(s, f_low, f_high):
        d1 = s + jnp.where(s >= 4, 2, 0)
        fits = (s >= 0) & (s < STEPS)

        @pl.when(fits & (z - d1 >= 0))
        def _():
            f_low(z - d1, d1)

        @pl.when(fits & (d1 > 0) & (z + d1 < NZ))
        def _():
            f_high(z + d1, d1)

        d2 = s + 2
        second = (s == 2) | (s == 3)

        @pl.when(second & (z - d2 >= 0))
        def _():
            f_low(z - d2, d2)

        @pl.when(second & (z + d2 < NZ))
        def _():
            f_high(z + d2, d2)

    z_up, z_down = jnp.minimum(z + 1, NZ - 1), jnp.maximum(z - 1, 0)
    z_far_up, z_far_down = jnp.minimum(z + EXPRESS, NZ - 1), jnp.maximum(z - EXPRESS, 0)

    def gather_copy(k, buf, zs, ys, half, link, arrival, to):
        blk = buf.at[zs, ys, half]
        return remote(blk, blk, ag_s.at[k, link], ag_r.at[k, arrival], to)

    DIRECT, RELAYED, UPWARD, DOWNWARD = 16, 17, 18, 34

    def even(v):
        return lax.rem(v, 2) == 0

    def arrived(k, buf, zs, half, arrival):
        gather_copy(k, buf, zs, y, half, 0, arrival, to_y(y_up)).wait_recv()

    def along_y(k, buf, zs, c, half):
        up = jnp.where(even(zs), 2 * zs + c, DIRECT)
        down = jnp.where(even(zs), DIRECT, 2 * zs + c)
        gather_copy(k, buf, zs, y, half, 0, up, to_y(y_up)).start()
        gather_copy(k, buf, zs, y, half, 0, down, to_y(y_down)).start()

    def gather_low(k, buf, zs, d):
        for c, half in HALVES:
            up, down = UPWARD + 2 * zs + c, DOWNWARD + 2 * zs + c

            @pl.when(d > 0)
            def _():
                arrived(k, buf, zs, half, up)

            @pl.when((z < NZ - 1) & (d != EXPRESS - 1))
            def _():
                gather_copy(k, buf, zs, y, half, 1, up, to_z(z_up)).start()

            @pl.when((d == 0) & (z > 0))
            def _():
                gather_copy(k, buf, zs, y, half, 1, down, to_z(z_down)).start()

            @pl.when((d == 0) & (z + EXPRESS < NZ))
            def _():
                gather_copy(k, buf, zs, y, half, 1, up, to_z(z_far_up)).start()

            @pl.when((d == 0) & (z - EXPRESS >= 0))
            def _():
                gather_copy(k, buf, zs, y, half, 1, down, to_z(z_far_down)).start()

            along_y(k, buf, zs, c, half)

    def gather_high(k, buf, zs, d):
        for c, half in HALVES:
            down = DOWNWARD + 2 * zs + c
            arrived(k, buf, zs, half, down)

            @pl.when((z > 0) & (d != EXPRESS - 1))
            def _():
                gather_copy(k, buf, zs, y, half, 1, down, to_z(z_down)).start()

            along_y(k, buf, zs, c, half)

    def gather_relay(k, buf, zs):
        origin = jnp.where(even(zs), y_down, y_up)
        onward = jnp.where(even(zs), y_up, y_down)
        for c, half in HALVES:
            arrived(k, buf, zs, half, 2 * zs + c)
            gather_copy(k, buf, zs, origin, half, 0, RELAYED, to_y(onward)).start()

    LAG = 2

    def gather_rounds(k, buf, first, last):
        def step(s, _):
            each(s, lambda zs, d: gather_low(k, buf, zs, d), lambda zs, d: gather_high(k, buf, zs, d))
            each(s - LAG, lambda zs, d: gather_relay(k, buf, zs), lambda zs, d: gather_relay(k, buf, zs))
            return 0

        lax.fori_loop(first, last, step, 0)

    def gather_end(k, buf):
        for arrival in (DIRECT, RELAYED):
            blocks = buf.at[:, y_far]
            remote(blocks, blocks, ag_s.at[k, 0], ag_r.at[k, arrival], to_y(y_up)).wait_recv()

    def wait_sent(sem, blocks):
        remote(blocks, blocks, sem, ag_r.at[0, 0], to_y(y_up)).wait_send()

    def gather_drain(k):
        wait_sent(ag_s.at[k, 0], ra.at[0:3])

        @pl.when((z == 0) | (z == 7))
        def _():
            wait_sent(ag_s.at[k, 1], ra.at[0, 0:2])

        @pl.when((z == 3) | (z == 4))
        def _():
            wait_sent(ag_s.at[k, 1], ra.at[0])

        @pl.when((z == 1) | (z == 2) | (z == 5) | (z == 6))
        def _():
            wait_sent(ag_s.at[k, 1], ra.at[0:3, 0:3])

    FAR, UP, DN, ZP, ZM, XP, XM = range(7)
    BOTH, CHAIN_UP, CHAIN_DOWN, FAR_UP, FAR_DOWN = 16, 32, 48, 64, 66

    def send_part(k, part, land, zd, col, half, link, kind, arrival, to):
        return remote(part.at[zd, col, half], land.at[kind, zd, half], rs_s.at[k, link], rs_r.at[k, arrival], to)

    def landed(k, land, kind, zd, half, arrival):
        blk = land.at[kind, zd] if half is None else land.at[kind, zd, half]
        remote(blk, blk, rs_s.at[k, 0], rs_r.at[k, arrival], to_y(y_up)).wait_recv()

    def wide(v):
        return v.astype(jnp.float32)

    def sum_far(k, part, land, zd):
        onward = jnp.where(even(zd), y_up, y_down)
        direct = jnp.where(even(zd), y_down, y_up)
        place = jnp.where(even(zd), DN, UP)
        for c, half in HALVES:
            send_part(k, part, land, zd, y_far, half, 0, FAR, 2 * zd + c, to_y(onward)).start()
            send_part(k, part, land, zd, direct, half, 0, place, BOTH + 2 * zd + c, to_y(direct)).start()

    def sum_near(k, part, land, zd):
        target = jnp.where(even(zd), y_up, y_down)
        place = jnp.where(even(zd), UP, DN)
        for c, half in HALVES:
            landed(k, land, FAR, zd, half, 2 * zd + c)
            part[zd, target, half] = (wide(part[zd, target, half]) + wide(land[FAR, zd, half])).astype(jnp.bfloat16)
            send_part(k, part, land, zd, target, half, 0, place, BOTH + 2 * zd + c, to_y(target)).start()

    def column_sum(k, part, land, zd, c, half):
        landed(k, land, UP, zd, None, BOTH + 2 * zd + c)
        return wide(part[zd, y, half]) + wide(land[UP, zd, half]) + wide(land[DN, zd, half])

    def sum_along_z(k, part, land, zd, d, chain, arrival, express, far_arrival, more, to_next, to_far):
        for c, half in HALVES:
            own = column_sum(k, part, land, zd, c, half)
            chained = more & (d != EXPRESS - 1)

            @pl.when(jnp.logical_not(chained))
            def _():
                part[zd, y, half] = own.astype(jnp.bfloat16)

            @pl.when(chained)
            def _():
                landed(k, land, chain, zd, half, arrival + 2 * zd + c)
                part[zd, y, half] = (own + wide(land[chain, zd, half])).astype(jnp.bfloat16)

            @pl.when(d != EXPRESS)
            def _():
                send_part(k, part, land, zd, y, half, 1, chain, arrival + 2 * zd + c, to_next).start()

            @pl.when(d == EXPRESS)
            def _():
                send_part(k, part, land, zd, y, half, 1, express, far_arrival + c, to_far).start()

    def sum_upward(k, part, land, zd, d):
        sum_along_z(k, part, land, zd, d, ZP, CHAIN_UP, XP, FAR_UP, z > 0, to_z(z_up), to_z(z_far_up))

    def sum_downward(k, part, land, zd, d):
        @pl.when(d > 0)
        def _():
            more = z < NZ - 1
            sum_along_z(k, part, land, zd, d, ZM, CHAIN_DOWN, XM, FAR_DOWN, more, to_z(z_down), to_z(z_far_down))

    def sum_result(k, part, land, own, give):
        def step(i, _):
            s = STEPS - 1 - i
            each(s, lambda zd, d: sum_far(k, part, land, zd), lambda zd, d: sum_far(k, part, land, zd))
            each(s + 1, lambda zd, d: sum_near(k, part, land, zd), lambda zd, d: sum_near(k, part, land, zd))
            each(
                s + 2,
                lambda zd, d: sum_downward(k, part, land, zd, d),
                lambda zd, d: sum_upward(k, part, land, zd, d),
            )
            return 0

        lax.fori_loop(0, STEPS + 1, step, 0)
        for c, half in HALVES:
            total = column_sum(k, part, land, z, c, half)
            for kind, there, arrival in (
                (ZP, z > 0, CHAIN_UP + 2 * z + c),
                (ZM, z < NZ - 1, CHAIN_DOWN + 2 * z + c),
                (XP, z - EXPRESS >= 0, FAR_UP + c),
                (XM, z + EXPRESS < NZ, FAR_DOWN + c),
            ):

                @pl.when(there)
                def _():
                    landed(k, land, kind, z, half, arrival)

                @pl.when(jnp.logical_not(there))
                def _():
                    land[kind, z, half] = jnp.zeros((32, TOK), jnp.bfloat16)

                total = total + wide(land[kind, z, half])
            give(half, (wide(own(half)) + 0.5 * FF ** (-0.5) * total).astype(jnp.bfloat16))

    def sum_drain(k, land):
        wait_sent(rs_s.at[k, 0], land.at[0:3])
        wait_sent(rs_s.at[k, 1], land.at[0, 0:7])

    def w1_copy(h, d):
        yd = wrap(y + d, NY)
        return remote(wp.at[h, yd], r1.at[h, pl.ds(y * 32, 32)], w1_s.at[h], w1_r.at[h], to_y(yd))

    def w1_start(h):
        for d in range(1, NY):
            w1_copy(h, d).start()

    def w1_wait(h):
        rows = r1.at[h, 0:96]
        remote(rows, rows, w1_s.at[h], w1_r.at[h], to_y(y_up)).wait_recv()

    def turn(h):
        turned = r1[h].astype(jnp.float32).T.astype(jnp.bfloat16)
        tt[h] = turned.reshape(3, NX, PART, 128)

    def w2_start(h):
        for d in range(1, NX):
            xd = wrap(x + d, NX)
            remote(tt.at[h, :, xd], r2.at[h, x], w2_s.at[h], w2_r.at[h], to_x(xd)).start()
        r2[h, x] = tt[h, :, x]

    def w2_wait(h):
        three = r2.at[h, 0:3]
        remote(three, three, w2_s.at[h], w2_r.at[h], to_x(x_up)).wait_recv()

    hub = core == lax.rem(z, 2)

    def part_rows(p):
        return pl.ds(pl.multiple_of(p * PART, 16), PART)

    def w3_columns():
        return pl.ds(pl.multiple_of(zz * 128, 128), 128)

    def w3_start(m):
        def step(i, _):
            target = lax.rem(i, 2) * NZ + (i // 2) * 2 + core

            @pl.when(target == zz)
            def _():
                wh[m, part_rows(x), w3_columns()] = r2[m // 3, i // 2, m % 3]

            @pl.when(target != zz)
            def _():
                block = wh.at[m, part_rows(x), w3_columns()]
                remote(r2.at[m // 3, i // 2, m % 3], block, w3_s.at[m // 3], w3_r.at[m], to_zz(target)).start()

            return 0

        lax.fori_loop(0, 2 * NX, step, 0)

    def w3_drain(h):
        @pl.when(hub)
        def _():
            wait_sent(w3_s.at[h], wh.at[0, 0 : 3 * PART, 0 : 7 * 128])

        @pl.when(jnp.logical_not(hub))
        def _():
            wait_sent(w3_s.at[h], wh.at[0, 0 : 3 * PART, 0 : 8 * 128])

    def w4_copy(m, kind, p, g, to):
        blk = wh.at[m, part_rows(p), pl.ds(g * GCOL, GCOL)]
        return remote(blk, blk, w4_s.at[0], w4_r.at[m, 4 if kind == 2 else 2 * kind + g], to)

    def w5_copy(m, p):
        blk = wh.at[m, part_rows(p)]
        return remote(blk, blk, w5_s.at[0], w5_r.at[m], sibling)

    def w4_send(m):
        @pl.when(hub)
        def _():
            others = wh.at[m, 0:PART, 0 : 15 * 128]
            remote(others, others, w3_s.at[0], w3_r.at[m], sibling).wait_recv()
            for g in range(NGRP):
                w4_copy(m, 0, x, g, to_x(x_up)).start()
                w4_copy(m, 1, x, g, to_x(x_down)).start()
            w5_copy(m, x).start()

    def w4_relay(m):
        @pl.when(hub)
        def _():
            for g in range(NGRP):
                w4_copy(m, 0, x_down, g, to_x(x_up)).wait_recv()
                if g % 2 == 0:
                    w4_copy(m, 2, x_down, g, to_x(x_up)).start()
                w4_copy(m, 1, x_up, g, to_x(x_down)).wait_recv()
                if g % 2 == 1:
                    w4_copy(m, 2, x_up, g, to_x(x_down)).start()
            w5_copy(m, x_down).start()
            w5_copy(m, x_up).start()

    def w5_send(m):
        @pl.when(hub)
        def _():
            far = wh.at[m, part_rows(x_far)]
            remote(far, far, w4_s.at[0], w4_r.at[m, 4], sibling).wait_recv()
            w5_copy(m, x_far).start()

    def w5_wait(m):
        @pl.when(jnp.logical_not(hub))
        def _():
            remote(wh.at[m], wh.at[m], w5_s.at[0], w5_r.at[m], sibling).wait_recv()

    def w_drain():
        for h in range(2):
            wait_sent(w1_s.at[h], wp.at[h, 0:3])
            wait_sent(w2_s.at[h], r2.at[h, 0:3])
            w3_drain(h)

        @pl.when(hub)
        def _():
            wait_sent(w4_s.at[0], wh.at[:, 0 : 3 * PART])
            wait_sent(w5_s.at[0], wh)

    def out_copy(m):
        return pltpu.make_async_copy(wh.at[m, pl.ds(0, WIDTH)], outs[m], out_s.at[m])

    def hidden_units(h, buf):
        whole = buf[...].reshape(D, TOK)
        wide_whole = whole.astype(jnp.float32)
        squares = jnp.sum(wide_whole * wide_whole, axis=0, keepdims=True)
        row_scale = lax.rsqrt(squares / D + norm_eps) * D ** (-0.5)
        g = jnp.dot(wh[3 * h, 0:WIDTH], whole, preferred_element_type=jnp.float32) * row_scale
        u = jnp.dot(wh[3 * h + 1, 0:WIDTH], whole, preferred_element_type=jnp.float32) * row_scale
        hid[...] = (g / (1.0 + jnp.exp(-g)) * u).astype(jnp.bfloat16)

    def partial_sums(h, part):
        def step(zd, _):
            w = wh[3 * h + 2, 0:WIDTH, pl.ds(pl.multiple_of(zd * 256, 256), 256)]
            p = lax.dot_general(w, hid[...], (((0,), (0,)), ((), ())), preferred_element_type=jnp.float32)
            part[zd] = p.astype(jnp.bfloat16).reshape(NY, FEAT, TOK)
            return 0

        lax.fori_loop(0, NZ, step, 0)

    w1_start(0)
    gather_rounds(0, xa, 0, 1)
    w1_start(1)
    gather_rounds(0, xa, 1, 2)
    w1_wait(0)
    turn(0)
    w2_start(0)
    gather_rounds(0, xa, 2, 3)
    w2_wait(0)
    for m in range(3):
        w3_start(m)
    gather_rounds(0, xa, 3, 5)
    w4_send(0)
    w1_wait(1)
    turn(1)
    w2_start(1)
    gather_rounds(0, xa, 5, 6)
    w4_relay(0)
    w4_send(1)
    gather_rounds(0, xa, 6, 7)
    w4_send(2)
    w4_relay(1)
    w5_send(0)
    gather_rounds(0, xa, 7, 8)
    w4_relay(2)
    w5_send(1)
    gather_end(0, xa)
    w5_send(2)
    w2_wait(1)
    for m in range(3, 6):
        w3_start(m)
    for m in range(2):
        w5_wait(m)
    hidden_units(0, xa)
    w5_wait(2)
    for m in range(3):
        out_copy(m).start()
    partial_sums(0, pa)

    def keep_middle(half, value):
        xb[z, y, half] = value

    def keep_result(half, value):
        res_ref[half] = value

    sum_result(0, pa, ra, lambda half: xa[z, y, half], keep_middle)
    gather_rounds(1, xb, 0, 1)
    for m in range(3, 6):
        w4_send(m)
    gather_rounds(1, xb, 1, 3)
    for m in range(3, 6):
        w4_relay(m)
    gather_rounds(1, xb, 3, STEPS)
    for m in range(3, 6):
        w5_send(m)
    gather_rounds(1, xb, STEPS, STEPS + LAG)
    gather_end(1, xb)
    for m in range(3, 6):
        w5_wait(m)
    for m in range(3, 6):
        out_copy(m).start()
    hidden_units(1, xb)
    partial_sums(1, pb)
    sum_result(1, pb, rb, lambda half: xb[z, y, half], keep_result)

    w_drain()
    for m in range(6):
        out_copy(m).wait()
    for k, land in ((0, ra), (1, rb)):
        gather_drain(k)
        sum_drain(k, land)


def write_out(*refs):
    ins, outs, held, sems = refs[:7], refs[7:14], refs[14:21], refs[21]
    loads = [pltpu.make_async_copy(ins[i], held[i], sems.at[0, i]) for i in range(7)]
    stores = [pltpu.make_async_copy(held[i], outs[i], sems.at[1, i]) for i in range(7)]
    for c in loads:
        c.start()
    for i in range(7):
        loads[i].wait()
        stores[i].start()
    for c in stores:
        c.wait()


def local(prompt, gain_pre, gate_pre, up_pre, down_pre, gain_post, gate_post, up_post, down_post):
    vm = pl.BlockSpec(memory_space=pltpu.VMEM)
    dma = pltpu.SemaphoreType.DMA
    bf = jnp.bfloat16
    hbm = pl.BlockSpec(memory_space=pltpu.HBM)
    shapes = (jax.ShapeDtypeStruct((FEAT, TOK), bf),) + (jax.ShapeDtypeStruct((WIDTH, D), bf),) * 6
    made = pl.pallas_call(
        kernel,
        out_shape=shapes,
        in_specs=[hbm] * 9,
        out_specs=(vm,) + (hbm,) * 6,
        scratch_shapes=[
            pltpu.VMEM((NZ, NY, FEAT, TOK), bf),
            pltpu.VMEM((NZ, NY, FEAT, TOK), bf),
            pltpu.VMEM((NZ, NY, FEAT, TOK), bf),
            pltpu.VMEM((NZ, NY, FEAT, TOK), bf),
            pltpu.VMEM((7, NZ, FEAT, TOK), bf),
            pltpu.VMEM((7, NZ, FEAT, TOK), bf),
            pltpu.VMEM((2, NY, 32, 3 * ROWS), bf),
            pltpu.VMEM((2, 128, 3 * ROWS), bf),
            pltpu.VMEM((2, 3, NX, PART, 128), bf),
            pltpu.VMEM((2, NX, 3, PART, 128), bf),
            pltpu.VMEM((6, ROWS, D), bf),
            pltpu.VMEM((2, 1, 32), jnp.float32),
            pltpu.VMEM((6, 32, NY * WIDTH), jnp.float32),
            pltpu.VMEM((WIDTH, TOK), bf),
            dma((2, 2)),
            dma((2, 50)),
            dma((2, 2)),
            dma((2, 68)),
            dma((2,)),
            dma((2,)),
            dma((2,)),
            dma((2,)),
            dma((2,)),
            dma((6,)),
            dma((1,)),
            dma((6, 5)),
            dma((1,)),
            dma((6,)),
            dma((9,)),
            dma((6,)),
        ],
        compiler_params=pltpu.CompilerParams(
            collective_id=0, has_side_effects=True, vmem_limit_bytes=58 * 1024 * 1024
        ),
    )(
        prompt.T,
        gain_pre.reshape(1, 32),
        gain_post.reshape(1, 32),
        gate_pre,
        up_pre,
        down_pre,
        gate_post,
        up_post,
        down_post,
    )
    res, *served = pl.pallas_call(
        write_out,
        out_shape=shapes,
        in_specs=[hbm] * 7,
        out_specs=(hbm,) * 7,
        scratch_shapes=[pltpu.VMEM(a.shape, bf) for a in shapes] + [dma((2, 7))],
    )(*made)
    return (res.T, *served)


def solution(mesh):
    rows = P(("gr", "fs"))
    block = P(("gr", "fs"), "tp")
    tokens = P(("gr", "tp"), "fs")
    return jax.shard_map(
        local,
        mesh=mesh,
        in_specs=(tokens, rows, block, block, block, rows, block, block, block),
        out_specs=(tokens,) + (P("fs", None),) * 6,
        check_vma=False,
    )
```

```python
import jax
import jax.numpy as jnp
from jax import lax
from jax.experimental import pallas as pl
from jax.experimental.pallas import tpu as pltpu
from jax.sharding import PartitionSpec as P

D = 2048
FF = 5632
NX, NY, NZ, NG = 4, 4, 8, 2
WIDTH = 176
FEAT = 64
TOK = 512
STREAM = TOK // 2
OFFSET = 0
PART = 48
ROWS = NX * PART
NGRP = 2
GCOL = D // NGRP
STRIDE = 3

norm_eps = 1e-06
MESH = pl.DeviceIdType.MESH


def kernel(
    x_ref, gain_a, gain_b, *refs
):
    mats, res_ref, outs = refs[:6], refs[6], refs[7:13]
    (xs_ref, part, land, wp, r1, r2, wh, gains, loaded, hid) = refs[13:23]
    (ag_s, ag_r, rs_s, rs_r, w1_s, w1_r, w3_s, w3_r, w4_s, w4_r, w5_s, w5_r, in_s, out_s) = refs[23:]

    gr, fs, tp = lax.axis_index("gr"), lax.axis_index("fs"), lax.axis_index("tp")
    y, z = lax.rem(fs, NY), fs // NY
    core, x = lax.rem(tp, 2), tp // 2
    zz = gr * NZ + z

    loads = [pltpu.make_async_copy(m, loaded.at[i], in_s.at[i]) for i, m in enumerate(mats)]
    loads.append(pltpu.make_async_copy(gain_a, gains.at[0], in_s.at[6]))
    loads.append(pltpu.make_async_copy(gain_b, gains.at[1], in_s.at[7]))
    for c in range(2):
        loads.append(pltpu.make_async_copy(x_ref.at[:, pl.ds(c * STREAM, STREAM)], xs_ref.at[0, c, z, y], in_s.at[8 + c]))
    for c in loads:
        c.start()

    def wrap(v, n):
        return lax.rem(v + n, n)

    def to_y(v):
        return {"fs": z * NY + v}

    def to_z(v):
        return {"fs": v * NY + y}

    def to_zz(v):
        return {"gr": v // NZ, "fs": lax.rem(v, NZ) * NY + y}

    def to_x(v):
        return {"tp": v * 2 + core}

    sibling = {"tp": x * 2 + 1 - core}
    y_up, y_down, y_far = wrap(y + 1, NY), wrap(y - 1, NY), wrap(y + 2, NY)
    x_up, x_down, x_far = wrap(x + 1, NX), wrap(x - 1, NX), wrap(x + 2, NX)

    def remote(src, dst, s, r, to):
        return pltpu.make_async_remote_copy(src, dst, s, r, device_id=to, device_id_type=MESH)

    barrier = pltpu.get_barrier_semaphore()

    def greet_z(i, _):
        pl.semaphore_signal(barrier, inc=1, device_id=to_zz(lax.rem(zz + i, NG * NZ)), device_id_type=MESH)
        return 0

    lax.fori_loop(1, NG * NZ, greet_z, 0)

    def to_plane(i):
        return {"fs": z * NY + lax.rem(y + i, NY), "tp": lax.rem(x + i // NY, NX) * 2 + core}

    def greet_plane(i, _):
        pl.semaphore_signal(barrier, inc=1, device_id=to_plane(i), device_id_type=MESH)
        return 0

    lax.fori_loop(1, NX * NY, greet_plane, 0)
    pl.semaphore_signal(barrier, inc=1, device_id=sibling, device_id_type=MESH)

    def pack(h):
        eye = lax.broadcasted_iota(jnp.int32, (32, 32), 0) == lax.broadcasted_iota(jnp.int32, (32, 32), 1)
        gain = jnp.sum(jnp.where(eye, jnp.broadcast_to(gains[h], (32, 32)), 0.0), axis=1, keepdims=True)
        three = [loaded[h * 3] * gain, loaded[h * 3 + 1] * gain, loaded[h * 3 + 2]]
        for at in range(NY):
            for p in range(NX):
                first, count = at * WIDTH + p * PART, min(PART, WIDTH - p * PART)
                pieces = [jnp.pad(v[:, first : first + count], ((0, 0), (0, PART - count))) for v in three]
                wp[h, p * NY + at] = jnp.concatenate(pieces, axis=1).astype(jnp.bfloat16)

    for c in loads:
        c.wait()
    pack(0)
    pack(1)
    for h in range(2):
        r1[h, x, pl.ds(y * 32, 32), :] = wp[h, x * NY + y]
    pl.semaphore_wait(barrier, NG * NZ - 1 + NX * NY - 1 + 1)

    STEPS = 5

    def each(s, f_low, f_high):
        d1 = s + jnp.where(s >= 3, 1, 0)
        fits = (s >= 0) & (s < STEPS)

        @pl.when(fits & (z - d1 >= 0))
        def _():
            f_low(z - d1, d1)

        @pl.when(fits & (d1 > 0) & (z + d1 < NZ))
        def _():
            f_high(z + d1, d1)

        d2 = s + jnp.where(s >= 3, 3, 1)
        second = (s >= 2) & (s < STEPS)

        @pl.when(second & (z - d2 >= 0))
        def _():
            f_low(z - d2, d2)

        @pl.when(second & (z + d2 < NZ))
        def _():
            f_high(z + d2, d2)

    z_up, z_down = jnp.minimum(z + 1, NZ - 1), jnp.maximum(z - 1, 0)
    far = (STRIDE, 2 * STRIDE)

    def up_by(d):
        return to_z(jnp.minimum(z + d, NZ - 1))

    def down_by(d):
        return to_z(jnp.maximum(z - d, 0))

    def chained(d):
        return lax.rem(d, STRIDE) != STRIDE - 1

    def gather_copy(k, c, zs, ys, link, arrival, to):
        blk = xs_ref.at[k, c, zs, ys]
        return remote(blk, blk, ag_s.at[2 * k + c, link], ag_r.at[2 * k + c, arrival], to)

    DIRECT, RELAYED, UPWARD, DOWNWARD = 8, 9, 10, 18

    def even(v):
        return lax.rem(v, 2) == 0

    def arrived(k, c, zs, arrival):
        gather_copy(k, c, zs, y, 0, arrival, to_y(y_up)).wait_recv()

    def along_y(k, c, zs):
        gather_copy(k, c, zs, y, 0, jnp.where(even(zs), zs, DIRECT), to_y(y_up)).start()
        gather_copy(k, c, zs, y, 0, jnp.where(even(zs), DIRECT, zs), to_y(y_down)).start()

    def gather_own(k, c):
        for d in reversed(far):

            @pl.when(z + d < NZ)
            def _():
                gather_copy(k, c, z, y, 1, UPWARD + z, up_by(d)).start()

            @pl.when(z - d >= 0)
            def _():
                gather_copy(k, c, z, y, 1, DOWNWARD + z, down_by(d)).start()

    def gather_low(k, c, zs, d):
        @pl.when(d > 0)
        def _():
            arrived(k, c, zs, UPWARD + zs)

        @pl.when((z < NZ - 1) & chained(d))
        def _():
            gather_copy(k, c, zs, y, 1, UPWARD + zs, to_z(z_up)).start()

        @pl.when((d == 0) & (z > 0))
        def _():
            gather_copy(k, c, zs, y, 1, DOWNWARD + zs, to_z(z_down)).start()

        along_y(k, c, zs)

    def gather_high(k, c, zs, d):
        arrived(k, c, zs, DOWNWARD + zs)

        @pl.when((z > 0) & chained(d))
        def _():
            gather_copy(k, c, zs, y, 1, DOWNWARD + zs, to_z(z_down)).start()

        along_y(k, c, zs)

    def gather_relay(k, c, zs):
        origin = jnp.where(even(zs), y_down, y_up)
        onward = jnp.where(even(zs), y_up, y_down)
        arrived(k, c, zs, zs)
        gather_copy(k, c, zs, origin, 0, RELAYED, to_y(onward)).start()

    LAG = 1

    def gather_tick(k, c, s):
        each(s, lambda zs, d: gather_low(k, c, zs, d), lambda zs, d: gather_high(k, c, zs, d))

        @pl.when(s == 0)
        def _():
            gather_own(k, c)

        each(s - LAG, lambda zs, d: gather_relay(k, c, zs), lambda zs, d: gather_relay(k, c, zs))

    def gather_end(k, c):
        for arrival in (DIRECT, RELAYED):
            blocks = land.at[0, 0, 0]
            remote(blocks, blocks, ag_s.at[2 * k + c, 0], ag_r.at[2 * k + c, arrival], to_y(y_up)).wait_recv()

    def wait_sent(sem, blocks):
        remote(blocks, blocks, sem, ag_r.at[0, 0], to_y(y_up)).wait_send()

    def gather_drain(j):
        wait_sent(ag_s.at[j, 0], land.at[0, 0, 0:3])

        @pl.when((z == 0) | (z == 7))
        def _():
            wait_sent(ag_s.at[j, 1], land.at[0, 0, 0, 0:3])

        @pl.when((z == 2) | (z == 5))
        def _():
            wait_sent(ag_s.at[j, 1], land.at[0, 0, 0, 0:7])

        @pl.when((z == 1) | (z == 3) | (z == 4) | (z == 6))
        def _():
            wait_sent(ag_s.at[j, 1], land.at[0, 0, 0:3, 0:3])

    FAR, UP, DN, ZP, ZM, XP, XM = 0, 1, 2, 3, 4, (5, 6), (7, 8)
    BOTH, CHAIN_UP, CHAIN_DOWN, FAR_UP, FAR_DOWN = 8, 16, 24, (32, 33), (34, 35)

    def send_part(k, c, zd, col, link, kind, arrival, to):
        there = land.at[k, c, kind, zd]
        return remote(part.at[k, c, zd, col], there, rs_s.at[2 * k + c, link], rs_r.at[2 * k + c, arrival], to)

    def landed(k, c, blk, arrival):
        remote(blk, blk, rs_s.at[2 * k + c, 0], rs_r.at[2 * k + c, arrival], to_y(y_up)).wait_recv()

    def wide(v):
        return v.astype(jnp.float32)

    def sum_far(k, c, zd):
        onward = jnp.where(even(zd), y_up, y_down)
        direct = jnp.where(even(zd), y_down, y_up)
        send_part(k, c, zd, y_far, 0, FAR, zd, to_y(onward)).start()
        send_part(k, c, zd, direct, 0, jnp.where(even(zd), DN, UP), BOTH + zd, to_y(direct)).start()

    def sum_near(k, c, zd):
        target = jnp.where(even(zd), y_up, y_down)
        landed(k, c, land.at[k, c, FAR, zd], zd)
        part[k, c, zd, target] = (wide(part[k, c, zd, target]) + wide(land[k, c, FAR, zd])).astype(jnp.bfloat16)
        send_part(k, c, zd, target, 0, jnp.where(even(zd), UP, DN), BOTH + zd, to_y(target)).start()

    def column_sum(k, c, zd):
        landed(k, c, land.at[k, c, UP, 0:2], BOTH + zd)
        return wide(part[k, c, zd, y]) + wide(land[k, c, UP, zd]) + wide(land[k, c, DN, zd])

    def sum_along_z(k, c, zd, d, chain, arrival, express, far_arrival, more, to_next, by):
        own = column_sum(k, c, zd)
        joined = more & chained(d)

        @pl.when(jnp.logical_not(joined))
        def _():
            part[k, c, zd, y] = own.astype(jnp.bfloat16)

        @pl.when(joined)
        def _():
            landed(k, c, land.at[k, c, chain, zd], arrival + zd)
            part[k, c, zd, y] = (own + wide(land[k, c, chain, zd])).astype(jnp.bfloat16)

        @pl.when(lax.rem(d, STRIDE) != 0)
        def _():
            send_part(k, c, zd, y, 1, chain, arrival + zd, to_next).start()

        for i in range(2):

            @pl.when(d == far[i])
            def _():
                send_part(k, c, zd, y, 1, express[i], far_arrival[i], by(far[i])).start()

    def sum_upward(k, c, zd, d):
        sum_along_z(k, c, zd, d, ZP, CHAIN_UP, XP, FAR_UP, z > 0, to_z(z_up), up_by)

    def sum_downward(k, c, zd, d):
        @pl.when(d > 0)
        def _():
            sum_along_z(k, c, zd, d, ZM, CHAIN_DOWN, XM, FAR_DOWN, z < NZ - 1, to_z(z_down), down_by)

    def partial_sum(k, c, zd):
        w = wh[3 * k + 2, 0:WIDTH, pl.ds(pl.multiple_of(zd * 256, 256), 256)]
        p = lax.dot_general(w, hid[c], (((0,), (0,)), ((), ())), preferred_element_type=jnp.float32)
        part[k, c, zd] = p.astype(jnp.bfloat16).reshape(NY, FEAT, STREAM)

    def sum_tick(k, c, i):
        s = STEPS - 1 - i

        def start(zd, d):
            partial_sum(k, c, zd)
            sum_far(k, c, zd)

        each(s, start, start)
        each(s + 1, lambda zd, d: sum_near(k, c, zd), lambda zd, d: sum_near(k, c, zd))
        each(s + 2, lambda zd, d: sum_downward(k, c, zd, d), lambda zd, d: sum_upward(k, c, zd, d))

    def sum_end(k, c):
        total = column_sum(k, c, z)
        for kind, there, arrival in (
            (ZP, z > 0, CHAIN_UP + z),
            (ZM, z < NZ - 1, CHAIN_DOWN + z),
            (XP[0], z - far[0] >= 0, FAR_UP[0]),
            (XP[1], z - far[1] >= 0, FAR_UP[1]),
            (XM[0], z + far[0] < NZ, FAR_DOWN[0]),
            (XM[1], z + far[1] < NZ, FAR_DOWN[1]),
        ):

            @pl.when(there)
            def _():
                landed(k, c, land.at[k, c, kind, z], arrival)

            @pl.when(jnp.logical_not(there))
            def _():
                land[k, c, kind, z] = jnp.zeros((FEAT, STREAM), jnp.bfloat16)

            total = total + wide(land[k, c, kind, z])
        value = (wide(xs_ref[k, c, z, y]) + 0.5 * FF ** (-0.5) * total).astype(jnp.bfloat16)

        @pl.when(k == 0)
        def _():
            xs_ref[1, c, z, y] = value

        @pl.when(k == 1)
        def _():
            res_ref[:, pl.ds(pl.multiple_of(c * STREAM, STREAM), STREAM)] = value

    def sum_drain(j):
        wait_sent(rs_s.at[j, 0], land.at[0, 0, 0:3])
        wait_sent(rs_s.at[j, 1], land.at[0, 0, 0, 0:7])

    def w1_start(h):
        def step(i, _):
            at = lax.rem(x + i // NY, NX) * NY + lax.rem(y + i, NY)
            rows = r1.at[h, x, pl.ds(y * 32, 32)]
            remote(wp.at[h, at], rows, w1_s.at[h], w1_r.at[h], to_plane(i)).start()
            return 0

        lax.fori_loop(1, NX * NY, step, 0)

    def w1_wait(h):
        others = wp.at[h, 0 : NX * NY - 1]
        remote(others, others, w1_s.at[h], w1_r.at[h], sibling).wait_recv()

    def turn(h):
        for xs in range(NX):
            r2[h, xs] = r1[h, xs].astype(jnp.float32).T.astype(jnp.bfloat16).reshape(3, PART, 128)

    hub = core == lax.rem(z, 2)

    def part_rows(p):
        return pl.ds(pl.multiple_of(p * PART, 16), PART)

    def w3_columns():
        return pl.ds(pl.multiple_of(zz * 128, 128), 128)

    def w3_start(m):
        def step(i, _):
            target = lax.rem(i, 2) * NZ + (i // 2) * 2 + core

            @pl.when(target == zz)
            def _():
                wh[m, part_rows(x), w3_columns()] = r2[m // 3, i // 2, m % 3]

            @pl.when(target != zz)
            def _():
                block = wh.at[m, part_rows(x), w3_columns()]
                remote(r2.at[m // 3, i // 2, m % 3], block, w3_s.at[m // 3], w3_r.at[m], to_zz(target)).start()

            return 0

        lax.fori_loop(0, 2 * NX, step, 0)

    def w3_drain(h):
        @pl.when(hub)
        def _():
            wait_sent(w3_s.at[h], wh.at[0, 0 : 3 * PART, 0 : 7 * 128])

        @pl.when(jnp.logical_not(hub))
        def _():
            wait_sent(w3_s.at[h], wh.at[0, 0 : 3 * PART, 0 : 8 * 128])

    def w4_copy(m, kind, p, g, to):
        blk = wh.at[m, part_rows(p), pl.ds(g * GCOL, GCOL)]
        return remote(blk, blk, w4_s.at[0], w4_r.at[m, 4 if kind == 2 else 2 * kind + g], to)

    def w5_copy(m, p):
        blk = wh.at[m, part_rows(p)]
        return remote(blk, blk, w5_s.at[0], w5_r.at[m], sibling)

    def w4_send(m):
        @pl.when(hub)
        def _():
            others = wh.at[m, 0:PART, 0 : 15 * 128]
            remote(others, others, w3_s.at[0], w3_r.at[m], sibling).wait_recv()
            for g in range(NGRP):
                w4_copy(m, 0, x, g, to_x(x_up)).start()
                w4_copy(m, 1, x, g, to_x(x_down)).start()
            w5_copy(m, x).start()

    def w4_relay(m):
        @pl.when(hub)
        def _():
            for g in range(NGRP):
                w4_copy(m, 0, x_down, g, to_x(x_up)).wait_recv()
                if g % 2 == 0:
                    w4_copy(m, 2, x_down, g, to_x(x_up)).start()
                w4_copy(m, 1, x_up, g, to_x(x_down)).wait_recv()
                if g % 2 == 1:
                    w4_copy(m, 2, x_up, g, to_x(x_down)).start()
            w5_copy(m, x_down).start()
            w5_copy(m, x_up).start()

    def w5_send(m):
        @pl.when(hub)
        def _():
            far = wh.at[m, part_rows(x_far)]
            remote(far, far, w4_s.at[0], w4_r.at[m, 4], sibling).wait_recv()
            w5_copy(m, x_far).start()

    def w5_wait(m):
        @pl.when(jnp.logical_not(hub))
        def _():
            remote(wh.at[m], wh.at[m], w5_s.at[0], w5_r.at[m], sibling).wait_recv()

    def w_drain():
        for h in range(2):
            wait_sent(w1_s.at[h], wp.at[h, 0 : NX * NY - 1])
            w3_drain(h)

        @pl.when(hub)
        def _():
            wait_sent(w4_s.at[0], wh.at[:, 0 : 3 * PART])
            wait_sent(w5_s.at[0], wh)

    def out_copy(m):
        return pltpu.make_async_copy(wh.at[m, pl.ds(0, WIDTH)], outs[m], out_s.at[m])

    def hidden_units(k, c):
        whole = xs_ref[k, c].reshape(D, STREAM)
        wide_whole = wide(whole)
        squares = jnp.sum(wide_whole * wide_whole, axis=0, keepdims=True)
        row_scale = lax.rsqrt(squares / D + norm_eps) * D ** (-0.5)
        g = jnp.dot(wh[3 * k, 0:WIDTH], whole, preferred_element_type=jnp.float32) * row_scale
        u = jnp.dot(wh[3 * k + 1, 0:WIDTH], whole, preferred_element_type=jnp.float32) * row_scale
        hid[c] = (g / (1.0 + jnp.exp(-g)) * u).astype(jnp.bfloat16)

    def both_streams(f):
        def step(c, _):
            f(c)
            return 0

        lax.fori_loop(0, 2, step, 0)

    def gather_rounds(first, last):
        def step(s, _):
            both_streams(lambda c: gather_tick(0, c, s))
            return 0

        lax.fori_loop(first, last, step, 0)

    w1_start(0)
    gather_rounds(0, 1)
    w1_wait(0)
    turn(0)
    for m in range(3):
        w3_start(m)
    gather_rounds(1, 2)
    w4_send(0)
    w1_start(1)
    gather_rounds(2, 3)
    w4_send(1)
    w4_relay(0)
    gather_rounds(3, 4)
    w4_send(2)
    w4_relay(1)
    w5_send(0)
    gather_rounds(4, 5)
    w4_relay(2)
    w5_send(1)
    gather_rounds(5, STEPS + LAG)
    w1_wait(1)
    turn(1)
    both_streams(lambda c: gather_end(0, c))
    w5_send(2)
    for m in range(3, 6):
        w3_start(m)
    for m in range(2):
        w5_wait(m)
    both_streams(lambda c: hidden_units(0, c))
    w5_wait(2)
    for m in range(3):
        out_copy(m).start()

    SUM = STEPS + 1
    GATHER = SUM + 1
    TURN = GATHER + STEPS + LAG
    AGAIN = TURN + 1
    LAST = AGAIN + SUM

    def tick(n, c):
        t = n - OFFSET * c

        @pl.when(((t >= 0) & (t < SUM)) | ((t >= AGAIN) & (t < LAST)))
        def _():
            k = jnp.where(t >= AGAIN, 1, 0)
            sum_tick(k, c, t - AGAIN * k)

        @pl.when((t == SUM) | (t == LAST))
        def _():
            sum_end(jnp.where(t == LAST, 1, 0), c)

        @pl.when((t >= GATHER) & (t < TURN))
        def _():
            gather_tick(1, c, t - GATHER)

        @pl.when(t == TURN)
        def _():
            gather_end(1, c)

            @pl.when(c == 0)
            def _():
                for m in range(3, 6):
                    w5_wait(m)
                for m in range(3, 6):
                    out_copy(m).start()

            hidden_units(1, c)

    def run(n, _):
        for at, act in ((SUM, w4_send), (GATHER + 2, w4_relay), (GATHER + 5, w5_send)):

            @pl.when(n == at)
            def _():
                for m in range(3, 6):
                    act(m)

        both_streams(lambda c: tick(n, c))
        return 0

    lax.fori_loop(0, LAST + OFFSET + 1, run, 0)

    w_drain()
    for m in range(6):
        out_copy(m).wait()
    for j in range(4):
        gather_drain(j)
        sum_drain(j)


def write_out(*refs):
    ins, outs, held, sems = refs[:7], refs[7:14], refs[14:21], refs[21]
    loads = [pltpu.make_async_copy(ins[i], held[i], sems.at[0, i]) for i in range(7)]
    stores = [pltpu.make_async_copy(held[i], outs[i], sems.at[1, i]) for i in range(7)]
    for c in loads:
        c.start()
    for i in range(7):
        loads[i].wait()
        stores[i].start()
    for c in stores:
        c.wait()


def local(prompt, gain_pre, gate_pre, up_pre, down_pre, gain_post, gate_post, up_post, down_post):
    vm = pl.BlockSpec(memory_space=pltpu.VMEM)
    dma = pltpu.SemaphoreType.DMA
    bf = jnp.bfloat16
    hbm = pl.BlockSpec(memory_space=pltpu.HBM)
    shapes = (jax.ShapeDtypeStruct((FEAT, TOK), bf),) + (jax.ShapeDtypeStruct((WIDTH, D), bf),) * 6
    made = pl.pallas_call(
        kernel,
        out_shape=shapes,
        in_specs=[hbm] * 9,
        out_specs=(vm,) + (hbm,) * 6,
        scratch_shapes=[
            pltpu.VMEM((2, 2, NZ, NY, FEAT, STREAM), bf),
            pltpu.VMEM((2, 2, NZ, NY, FEAT, STREAM), bf),
            pltpu.VMEM((2, 2, 9, NZ, FEAT, STREAM), bf),
            pltpu.VMEM((2, NX * NY, 32, 3 * PART), bf),
            pltpu.VMEM((2, NX, 128, 3 * PART), bf),
            pltpu.VMEM((2, NX, 3, PART, 128), bf),
            pltpu.VMEM((6, ROWS, D), bf),
            pltpu.VMEM((2, 1, 32), jnp.float32),
            pltpu.VMEM((6, 32, NY * WIDTH), jnp.float32),
            pltpu.VMEM((2, WIDTH, STREAM), bf),
            dma((4, 2)),
            dma((4, 26)),
            dma((4, 2)),
            dma((4, 36)),
            dma((2,)),
            dma((2,)),
            dma((2,)),
            dma((6,)),
            dma((1,)),
            dma((6, 5)),
            dma((1,)),
            dma((6,)),
            dma((10,)),
            dma((6,)),
        ],
        compiler_params=pltpu.CompilerParams(
            collective_id=0, has_side_effects=True, vmem_limit_bytes=58 * 1024 * 1024
        ),
    )(
        prompt.T,
        gain_pre.reshape(1, 32),
        gain_post.reshape(1, 32),
        gate_pre,
        up_pre,
        down_pre,
        gate_post,
        up_post,
        down_post,
    )
    res, *served = pl.pallas_call(
        write_out,
        out_shape=shapes,
        in_specs=[hbm] * 7,
        out_specs=(hbm,) * 7,
        scratch_shapes=[pltpu.VMEM(a.shape, bf) for a in shapes] + [dma((2, 7))],
    )(*made)
    return (res.T, *served)


def solution(mesh):
    rows = P(("gr", "fs"))
    block = P(("gr", "fs"), "tp")
    tokens = P(("gr", "tp"), "fs")
    return jax.shard_map(
        local,
        mesh=mesh,
        in_specs=(tokens, rows, block, block, block, rows, block, block, block),
        out_specs=(tokens,) + (P("fs", None),) * 6,
        check_vma=False,
    )
```

```python
import jax
import jax.numpy as jnp
from jax import lax
from jax.experimental import pallas as pl
from jax.experimental.pallas import tpu as pltpu
from jax.sharding import PartitionSpec as P

D = 2048
FF = 5632
NX, NY, NZ, NG = 4, 4, 8, 2
WIDTH = 176
FEAT = 64
TOK = 512
STREAM = TOK // 2
OFFSET = 0
PART = 48
ROWS = NX * PART
NGRP = 2
GCOL = D // NGRP
STRIDE = 3

norm_eps = 1e-06
MESH = pl.DeviceIdType.MESH


def kernel(
    x_ref, gain_a, gain_b, *refs
):
    mats, res_ref, outs = refs[:6], refs[6], refs[7:13]
    (xs_ref, part, land, wp, r1, r2, wh, gains, loaded, hid) = refs[13:23]
    (ag_s, ag_r, rs_s, rs_r, w1_s, w1_r, w3_s, w3_r, w4_s, w4_r, w5_s, w5_r, in_s, out_s) = refs[23:]

    gr, fs, tp = lax.axis_index("gr"), lax.axis_index("fs"), lax.axis_index("tp")
    y, z = lax.rem(fs, NY), fs // NY
    core, x = lax.rem(tp, 2), tp // 2
    zz = gr * NZ + z

    loads = [pltpu.make_async_copy(m, loaded.at[i], in_s.at[i]) for i, m in enumerate(mats)]
    loads.append(pltpu.make_async_copy(gain_a, gains.at[0], in_s.at[6]))
    loads.append(pltpu.make_async_copy(gain_b, gains.at[1], in_s.at[7]))
    for c in range(2):
        loads.append(pltpu.make_async_copy(x_ref.at[:, pl.ds(c * STREAM, STREAM)], xs_ref.at[0, c, z, y], in_s.at[8 + c]))
    for c in loads:
        c.start()

    def wrap(v, n):
        return lax.rem(v + n, n)

    def to_y(v):
        return {"fs": z * NY + v}

    def to_z(v):
        return {"fs": v * NY + y}

    def to_zz(v):
        return {"gr": v // NZ, "fs": lax.rem(v, NZ) * NY + y}

    def to_x(v):
        return {"tp": v * 2 + core}

    sibling = {"tp": x * 2 + 1 - core}
    y_up, y_down, y_far = wrap(y + 1, NY), wrap(y - 1, NY), wrap(y + 2, NY)
    x_up, x_down, x_far = wrap(x + 1, NX), wrap(x - 1, NX), wrap(x + 2, NX)

    def remote(src, dst, s, r, to):
        return pltpu.make_async_remote_copy(src, dst, s, r, device_id=to, device_id_type=MESH)

    barrier = pltpu.get_barrier_semaphore()

    def greet_z(i, _):
        pl.semaphore_signal(barrier, inc=1, device_id=to_zz(lax.rem(zz + i, NG * NZ)), device_id_type=MESH)
        return 0

    lax.fori_loop(1, NG * NZ, greet_z, 0)

    def to_plane(i):
        return {"fs": z * NY + lax.rem(y + i, NY), "tp": lax.rem(x + i // NY, NX) * 2 + core}

    def greet_plane(i, _):
        pl.semaphore_signal(barrier, inc=1, device_id=to_plane(i), device_id_type=MESH)
        return 0

    lax.fori_loop(1, NX * NY, greet_plane, 0)
    pl.semaphore_signal(barrier, inc=1, device_id=sibling, device_id_type=MESH)

    def pack(h):
        eye = lax.broadcasted_iota(jnp.int32, (32, 32), 0) == lax.broadcasted_iota(jnp.int32, (32, 32), 1)
        gain = jnp.sum(jnp.where(eye, jnp.broadcast_to(gains[h], (32, 32)), 0.0), axis=1, keepdims=True)
        three = [loaded[h * 3] * gain, loaded[h * 3 + 1] * gain, loaded[h * 3 + 2]]
        for at in range(NY):
            for p in range(NX):
                first, count = at * WIDTH + p * PART, min(PART, WIDTH - p * PART)
                pieces = [jnp.pad(v[:, first : first + count], ((0, 0), (0, PART - count))) for v in three]
                wp[h, p * NY + at] = jnp.concatenate(pieces, axis=1).astype(jnp.bfloat16)

    for c in loads:
        c.wait()
    pack(0)
    pack(1)
    for h in range(2):
        r1[h, x, pl.ds(y * 32, 32), :] = wp[h, x * NY + y]
    pl.semaphore_wait(barrier, NG * NZ - 1 + NX * NY - 1 + 1)

    STEPS = 5

    def each(s, f_low, f_high):
        d1 = s + jnp.where(s >= 3, 1, 0)
        fits = (s >= 0) & (s < STEPS)

        @pl.when(fits & (z - d1 >= 0))
        def _():
            f_low(z - d1, d1)

        @pl.when(fits & (d1 > 0) & (z + d1 < NZ))
        def _():
            f_high(z + d1, d1)

        d2 = s + jnp.where(s >= 3, 3, 1)
        second = (s >= 2) & (s < STEPS)

        @pl.when(second & (z - d2 >= 0))
        def _():
            f_low(z - d2, d2)

        @pl.when(second & (z + d2 < NZ))
        def _():
            f_high(z + d2, d2)

    z_up, z_down = jnp.minimum(z + 1, NZ - 1), jnp.maximum(z - 1, 0)
    far = (STRIDE, 2 * STRIDE)

    def up_by(d):
        return to_z(jnp.minimum(z + d, NZ - 1))

    def down_by(d):
        return to_z(jnp.maximum(z - d, 0))

    def chained(d):
        return lax.rem(d, STRIDE) != STRIDE - 1

    def gather_copy(k, c, zs, ys, link, arrival, to):
        blk = xs_ref.at[k, c, zs, ys]
        return remote(blk, blk, ag_s.at[2 * k + c, link], ag_r.at[c, arrival], to)

    DIRECT, RELAYED, UPWARD, DOWNWARD = 8, 9, 10, 10

    def even(v):
        return lax.rem(v, 2) == 0

    def arrived(k, c, zs, arrival):
        gather_copy(k, c, zs, y, 0, arrival, to_y(y_up)).wait_recv()

    def along_y(k, c, zs):
        gather_copy(k, c, zs, y, 0, jnp.where(even(zs), zs, DIRECT), to_y(y_up)).start()
        gather_copy(k, c, zs, y, 0, jnp.where(even(zs), DIRECT, zs), to_y(y_down)).start()

    def gather_own(k, c):
        for d in reversed(far):

            @pl.when(z + d < NZ)
            def _():
                gather_copy(k, c, z, y, 1, UPWARD + z, up_by(d)).start()

            @pl.when(z - d >= 0)
            def _():
                gather_copy(k, c, z, y, 1, DOWNWARD + z, down_by(d)).start()

    def gather_low(k, c, zs, d):
        @pl.when(d > 0)
        def _():
            arrived(k, c, zs, UPWARD + zs)

        @pl.when((z < NZ - 1) & chained(d))
        def _():
            gather_copy(k, c, zs, y, 1, UPWARD + zs, to_z(z_up)).start()

        @pl.when((d == 0) & (z > 0))
        def _():
            gather_copy(k, c, zs, y, 1, DOWNWARD + zs, to_z(z_down)).start()

        along_y(k, c, zs)

    def gather_high(k, c, zs, d):
        arrived(k, c, zs, DOWNWARD + zs)

        @pl.when((z > 0) & chained(d))
        def _():
            gather_copy(k, c, zs, y, 1, DOWNWARD + zs, to_z(z_down)).start()

        along_y(k, c, zs)

    def gather_relay(k, c, zs):
        origin = jnp.where(even(zs), y_down, y_up)
        onward = jnp.where(even(zs), y_up, y_down)
        arrived(k, c, zs, zs)
        gather_copy(k, c, zs, origin, 0, RELAYED, to_y(onward)).start()

    LAG = 1

    def gather_tick(k, c, s):
        each(s, lambda zs, d: gather_low(k, c, zs, d), lambda zs, d: gather_high(k, c, zs, d))

        @pl.when(s == 0)
        def _():
            gather_own(k, c)

        each(s - LAG, lambda zs, d: gather_relay(k, c, zs), lambda zs, d: gather_relay(k, c, zs))

    def gather_end(k, c):
        for arrival in (DIRECT, RELAYED):
            blocks = land.at[0, 0, 0]
            remote(blocks, blocks, ag_s.at[2 * k + c, 0], ag_r.at[c, arrival], to_y(y_up)).wait_recv()

    def wait_sent(sem, blocks):
        remote(blocks, blocks, sem, ag_r.at[0, 0], to_y(y_up)).wait_send()

    def gather_drain(j):
        wait_sent(ag_s.at[j, 0], land.at[0, 0, 0:3])

        @pl.when((z == 0) | (z == 7))
        def _():
            wait_sent(ag_s.at[j, 1], land.at[0, 0, 0, 0:3])

        @pl.when((z == 2) | (z == 5))
        def _():
            wait_sent(ag_s.at[j, 1], land.at[0, 0, 0, 0:7])

        @pl.when((z == 1) | (z == 3) | (z == 4) | (z == 6))
        def _():
            wait_sent(ag_s.at[j, 1], land.at[0, 0, 0:3, 0:3])

    FAR, UP, DN, ZP, ZM, XP, XM = 0, 1, 2, 3, 4, (5, 6), (7, 8)
    BOTH, CHAIN_UP, CHAIN_DOWN, FAR_UP, FAR_DOWN = 8, 16, 24, (32, 33), (34, 35)

    def send_part(k, c, zd, col, link, kind, arrival, to):
        there = land.at[k, c, kind, zd]
        return remote(part.at[k, c, zd, col], there, rs_s.at[2 * k + c, link], rs_r.at[c, arrival], to)

    def landed(k, c, blk, arrival):
        remote(blk, blk, rs_s.at[2 * k + c, 0], rs_r.at[c, arrival], to_y(y_up)).wait_recv()

    def wide(v):
        return v.astype(jnp.float32)

    def sum_far(k, c, zd):
        onward = jnp.where(even(zd), y_up, y_down)
        direct = jnp.where(even(zd), y_down, y_up)
        send_part(k, c, zd, y_far, 0, FAR, zd, to_y(onward)).start()
        send_part(k, c, zd, direct, 0, jnp.where(even(zd), DN, UP), BOTH + zd, to_y(direct)).start()

    def sum_near(k, c, zd):
        target = jnp.where(even(zd), y_up, y_down)
        landed(k, c, land.at[k, c, FAR, zd], zd)
        part[k, c, zd, target] = (wide(part[k, c, zd, target]) + wide(land[k, c, FAR, zd])).astype(jnp.bfloat16)
        send_part(k, c, zd, target, 0, jnp.where(even(zd), UP, DN), BOTH + zd, to_y(target)).start()

    def column_sum(k, c, zd):
        landed(k, c, land.at[k, c, UP, 0:2], BOTH + zd)
        return wide(part[k, c, zd, y]) + wide(land[k, c, UP, zd]) + wide(land[k, c, DN, zd])

    def sum_along_z(k, c, zd, d, chain, arrival, express, far_arrival, more, to_next, by):
        own = column_sum(k, c, zd)
        joined = more & chained(d)

        @pl.when(jnp.logical_not(joined))
        def _():
            part[k, c, zd, y] = own.astype(jnp.bfloat16)

        @pl.when(joined)
        def _():
            landed(k, c, land.at[k, c, chain, zd], arrival + zd)
            part[k, c, zd, y] = (own + wide(land[k, c, chain, zd])).astype(jnp.bfloat16)

        @pl.when(lax.rem(d, STRIDE) != 0)
        def _():
            send_part(k, c, zd, y, 1, chain, arrival + zd, to_next).start()

        for i in range(2):

            @pl.when(d == far[i])
            def _():
                send_part(k, c, zd, y, 1, express[i], far_arrival[i], by(far[i])).start()

    def sum_upward(k, c, zd, d):
        sum_along_z(k, c, zd, d, ZP, CHAIN_UP, XP, FAR_UP, z > 0, to_z(z_up), up_by)

    def sum_downward(k, c, zd, d):
        @pl.when(d > 0)
        def _():
            sum_along_z(k, c, zd, d, ZM, CHAIN_DOWN, XM, FAR_DOWN, z < NZ - 1, to_z(z_down), down_by)

    def partial_sum(k, c, zd):
        w = wh[3 * k + 2, 0:WIDTH, pl.ds(pl.multiple_of(zd * 256, 256), 256)]
        p = lax.dot_general(w, hid[c], (((0,), (0,)), ((), ())), preferred_element_type=jnp.float32)
        part[k, c, zd] = p.astype(jnp.bfloat16).reshape(NY, FEAT, STREAM)

    def sum_tick(k, c, i):
        s = STEPS - 1 - i

        def start(zd, d):
            partial_sum(k, c, zd)
            sum_far(k, c, zd)

        each(s, start, start)
        each(s + 1, lambda zd, d: sum_near(k, c, zd), lambda zd, d: sum_near(k, c, zd))
        each(s + 2, lambda zd, d: sum_downward(k, c, zd, d), lambda zd, d: sum_upward(k, c, zd, d))

    def sum_end(k, c):
        total = column_sum(k, c, z)
        for kind, there, arrival in (
            (ZP, z > 0, CHAIN_UP + z),
            (ZM, z < NZ - 1, CHAIN_DOWN + z),
            (XP[0], z - far[0] >= 0, FAR_UP[0]),
            (XP[1], z - far[1] >= 0, FAR_UP[1]),
            (XM[0], z + far[0] < NZ, FAR_DOWN[0]),
            (XM[1], z + far[1] < NZ, FAR_DOWN[1]),
        ):

            @pl.when(there)
            def _():
                landed(k, c, land.at[k, c, kind, z], arrival)

            @pl.when(jnp.logical_not(there))
            def _():
                land[k, c, kind, z] = jnp.zeros((FEAT, STREAM), jnp.bfloat16)

            total = total + wide(land[k, c, kind, z])
        value = (wide(xs_ref[k, c, z, y]) + 0.5 * FF ** (-0.5) * total).astype(jnp.bfloat16)

        @pl.when(k == 0)
        def _():
            xs_ref[1, c, z, y] = value

        @pl.when(k == 1)
        def _():
            res_ref[:, pl.ds(pl.multiple_of(c * STREAM, STREAM), STREAM)] = value

    def sum_drain(j):
        wait_sent(rs_s.at[j, 0], land.at[0, 0, 0:3])
        wait_sent(rs_s.at[j, 1], land.at[0, 0, 0, 0:7])

    def w1_start(h):
        def step(i, _):
            at = lax.rem(x + i // NY, NX) * NY + lax.rem(y + i, NY)
            rows = r1.at[h, x, pl.ds(y * 32, 32)]
            remote(wp.at[h, at], rows, w1_s.at[h], w1_r.at[h], to_plane(i)).start()
            return 0

        lax.fori_loop(1, NX * NY, step, 0)

    def w1_wait(h):
        others = wp.at[h, 0 : NX * NY - 1]
        remote(others, others, w1_s.at[h], w1_r.at[h], sibling).wait_recv()

    def turn(h):
        for xs in range(NX):
            r2[h, xs] = r1[h, xs].astype(jnp.float32).T.astype(jnp.bfloat16).reshape(3, PART, 128)

    hub = core == lax.rem(z, 2)

    def part_rows(p):
        return pl.ds(pl.multiple_of(p * PART, 16), PART)

    def w3_columns():
        return pl.ds(pl.multiple_of(zz * 128, 128), 128)

    def w3_start(m):
        def step(i, _):
            target = lax.rem(i, 2) * NZ + (i // 2) * 2 + core

            @pl.when(target == zz)
            def _():
                wh[m, part_rows(x), w3_columns()] = r2[m // 3, i // 2, m % 3]

            @pl.when(target != zz)
            def _():
                block = wh.at[m, part_rows(x), w3_columns()]
                remote(r2.at[m // 3, i // 2, m % 3], block, w3_s.at[m // 3], w3_r.at[m], to_zz(target)).start()

            return 0

        lax.fori_loop(0, 2 * NX, step, 0)

    def w3_drain(h):
        @pl.when(hub)
        def _():
            wait_sent(w3_s.at[h], wh.at[0, 0 : 3 * PART, 0 : 7 * 128])

        @pl.when(jnp.logical_not(hub))
        def _():
            wait_sent(w3_s.at[h], wh.at[0, 0 : 3 * PART, 0 : 8 * 128])

    def w4_copy(m, kind, p, g, to):
        blk = wh.at[m, part_rows(p), pl.ds(g * GCOL, GCOL)]
        return remote(blk, blk, w4_s.at[0], w4_r.at[m, 4 if kind == 2 else 2 * kind + g], to)

    def w5_copy(m, p):
        blk = wh.at[m, part_rows(p)]
        return remote(blk, blk, w5_s.at[0], w5_r.at[m], sibling)

    def w4_send(m):
        @pl.when(hub)
        def _():
            others = wh.at[m, 0:PART, 0 : 15 * 128]
            remote(others, others, w3_s.at[0], w3_r.at[m], sibling).wait_recv()
            for g in range(NGRP):
                w4_copy(m, 0, x, g, to_x(x_up)).start()
                w4_copy(m, 1, x, g, to_x(x_down)).start()
            w5_copy(m, x).start()

    def w4_relay(m):
        @pl.when(hub)
        def _():
            for g in range(NGRP):
                w4_copy(m, 0, x_down, g, to_x(x_up)).wait_recv()
                if g % 2 == 0:
                    w4_copy(m, 2, x_down, g, to_x(x_up)).start()
                w4_copy(m, 1, x_up, g, to_x(x_down)).wait_recv()
                if g % 2 == 1:
                    w4_copy(m, 2, x_up, g, to_x(x_down)).start()
            w5_copy(m, x_down).start()
            w5_copy(m, x_up).start()

    def w5_send(m):
        @pl.when(hub)
        def _():
            far = wh.at[m, part_rows(x_far)]
            remote(far, far, w4_s.at[0], w4_r.at[m, 4], sibling).wait_recv()
            w5_copy(m, x_far).start()

    def w5_wait(m):
        @pl.when(jnp.logical_not(hub))
        def _():
            remote(wh.at[m], wh.at[m], w5_s.at[0], w5_r.at[m], sibling).wait_recv()

    def w_drain():
        for h in range(2):
            wait_sent(w1_s.at[h], wp.at[h, 0 : NX * NY - 1])
            w3_drain(h)

        @pl.when(hub)
        def _():
            wait_sent(w4_s.at[0], wh.at[:, 0 : 3 * PART])
            wait_sent(w5_s.at[0], wh)

    def out_copy(m):
        return pltpu.make_async_copy(wh.at[m, pl.ds(0, WIDTH)], outs[m], out_s.at[m])

    def hidden_units(k, c):
        whole = xs_ref[k, c].reshape(D, STREAM)
        wide_whole = wide(whole)
        squares = jnp.sum(wide_whole * wide_whole, axis=0, keepdims=True)
        row_scale = lax.rsqrt(squares / D + norm_eps) * D ** (-0.5)
        g = jnp.dot(wh[3 * k, 0:WIDTH], whole, preferred_element_type=jnp.float32) * row_scale
        u = jnp.dot(wh[3 * k + 1, 0:WIDTH], whole, preferred_element_type=jnp.float32) * row_scale
        hid[c] = (g / (1.0 + jnp.exp(-g)) * u).astype(jnp.bfloat16)

    def both_streams(f):
        def step(c, _):
            f(c)
            return 0

        lax.fori_loop(0, 2, step, 0)

    def gather_rounds(first, last):
        def step(s, _):
            both_streams(lambda c: gather_tick(0, c, s))
            return 0

        lax.fori_loop(first, last, step, 0)

    w1_start(0)
    gather_rounds(0, 1)
    w1_wait(0)
    turn(0)
    for m in range(3):
        w3_start(m)
    w1_start(1)
    gather_rounds(1, 2)
    w4_send(0)
    gather_rounds(2, 3)
    w4_send(1)
    w4_relay(0)
    gather_rounds(3, 4)
    w4_send(2)
    w4_relay(1)
    w5_send(0)
    gather_rounds(4, 5)
    w4_relay(2)
    w5_send(1)
    w1_wait(1)
    turn(1)
    for m in range(3, 6):
        w3_start(m)
    gather_rounds(5, STEPS + LAG)
    both_streams(lambda c: gather_end(0, c))
    w5_send(2)
    for m in range(2):
        w5_wait(m)
    both_streams(lambda c: hidden_units(0, c))
    w5_wait(2)
    for m in range(3):
        out_copy(m).start()

    SUM = STEPS + 1
    GATHER = SUM + 1
    TURN = GATHER + STEPS + LAG
    AGAIN = TURN + 1
    LAST = AGAIN + SUM

    def tick(n, c):
        t = n - OFFSET * c

        @pl.when(((t >= 0) & (t < SUM)) | ((t >= AGAIN) & (t < LAST)))
        def _():
            k = jnp.where(t >= AGAIN, 1, 0)
            sum_tick(k, c, t - AGAIN * k)

        @pl.when((t == SUM) | (t == LAST))
        def _():
            sum_end(jnp.where(t == LAST, 1, 0), c)

        @pl.when((t >= GATHER) & (t < TURN))
        def _():
            gather_tick(1, c, t - GATHER)

        @pl.when(t == TURN)
        def _():
            gather_end(1, c)

            @pl.when(c == 0)
            def _():
                for m in range(3, 6):
                    w5_wait(m)
                for m in range(3, 6):
                    out_copy(m).start()

            hidden_units(1, c)

    def run(n, _):
        for at, act in ((SUM, w4_send), (GATHER + 2, w4_relay), (GATHER + 5, w5_send)):

            @pl.when(n == at)
            def _():
                for m in range(3, 6):
                    act(m)

        both_streams(lambda c: tick(n, c))
        return 0

    lax.fori_loop(0, LAST + OFFSET + 1, run, 0)

    w_drain()
    for m in range(6):
        out_copy(m).wait()
    for j in range(4):
        gather_drain(j)
        sum_drain(j)


def write_out(*refs):
    ins, outs, held, sems = refs[:7], refs[7:14], refs[14:21], refs[21]
    loads = [pltpu.make_async_copy(ins[i], held[i], sems.at[0, i]) for i in range(7)]
    stores = [pltpu.make_async_copy(held[i], outs[i], sems.at[1, i]) for i in range(7)]
    for c in loads:
        c.start()
    for i in range(7):
        loads[i].wait()
        stores[i].start()
    for c in stores:
        c.wait()


def local(prompt, gain_pre, gate_pre, up_pre, down_pre, gain_post, gate_post, up_post, down_post):
    vm = pl.BlockSpec(memory_space=pltpu.VMEM)
    dma = pltpu.SemaphoreType.DMA
    bf = jnp.bfloat16
    hbm = pl.BlockSpec(memory_space=pltpu.HBM)
    shapes = (jax.ShapeDtypeStruct((FEAT, TOK), bf),) + (jax.ShapeDtypeStruct((WIDTH, D), bf),) * 6
    made = pl.pallas_call(
        kernel,
        out_shape=shapes,
        in_specs=[hbm] * 9,
        out_specs=(vm,) + (hbm,) * 6,
        scratch_shapes=[
            pltpu.VMEM((2, 2, NZ, NY, FEAT, STREAM), bf),
            pltpu.VMEM((2, 2, NZ, NY, FEAT, STREAM), bf),
            pltpu.VMEM((2, 2, 9, NZ, FEAT, STREAM), bf),
            pltpu.VMEM((2, NX * NY, 32, 3 * PART), bf),
            pltpu.VMEM((2, NX, 128, 3 * PART), bf),
            pltpu.VMEM((2, NX, 3, PART, 128), bf),
            pltpu.VMEM((6, ROWS, D), bf),
            pltpu.VMEM((2, 1, 32), jnp.float32),
            pltpu.VMEM((6, 32, NY * WIDTH), jnp.float32),
            pltpu.VMEM((2, WIDTH, STREAM), bf),
            dma((4, 2)),
            dma((2, 18)),
            dma((4, 2)),
            dma((2, 36)),
            dma((2,)),
            dma((2,)),
            dma((2,)),
            dma((6,)),
            dma((1,)),
            dma((6, 5)),
            dma((1,)),
            dma((6,)),
            dma((10,)),
            dma((6,)),
        ],
        compiler_params=pltpu.CompilerParams(
            collective_id=0, has_side_effects=True, vmem_limit_bytes=58 * 1024 * 1024
        ),
    )(
        prompt.T,
        gain_pre.reshape(1, 32),
        gain_post.reshape(1, 32),
        gate_pre,
        up_pre,
        down_pre,
        gate_post,
        up_post,
        down_post,
    )
    res, *served = pl.pallas_call(
        write_out,
        out_shape=shapes,
        in_specs=[hbm] * 7,
        out_specs=(hbm,) * 7,
        scratch_shapes=[pltpu.VMEM(a.shape, bf) for a in shapes] + [dma((2, 7))],
    )(*made)
    return (res.T, *served)


def solution(mesh):
    rows = P(("gr", "fs"))
    block = P(("gr", "fs"), "tp")
    tokens = P(("gr", "tp"), "fs")
    return jax.shard_map(
        local,
        mesh=mesh,
        in_specs=(tokens, rows, block, block, block, rows, block, block, block),
        out_specs=(tokens,) + (P("fs", None),) * 6,
        check_vma=False,
    )
```
